256 devices in a mesh: sp: 32 (over z, y), tp: 8 (over x, core).
Axes of the slice: x: 4, y: 4, z: 8, core: 2. Of those that a mesh axis runs over, the one named last changes fastest.
Arguments:
- activations: bfloat16 [24576, 2048], P(('sp', 'tp')), may hold values from -6 to 6
- in_gain: float32 [2048], replicated, may hold values from 0.1 to 1.9
- w_pool_in: bfloat16 [2048, 1024], P(None, 'tp'), may hold values from -0.125 to 0.125
- pool_gain: float32 [1024], P('tp'), may hold values from 0.1 to 1.9
- w_qlat: bfloat16 [2048, 768], P(None, 'tp'), may hold values from -0.125 to 0.125
- w_kvlat: bfloat16 [2048, 512], P(None, 'tp'), may hold values from -0.125 to 0.125
- w_krope: bfloat16 [2048, 32], replicated, may hold values from -0.125 to 0.125
- qlat_gain: float32 [768], replicated, may hold values from 0.1 to 1.9
- kvlat_gain: float32 [512], replicated, may hold values from 0.1 to 1.9
- w_qup: bfloat16 [768, 1536], P(None, 'tp'), may hold values from -0.21875 to 0.21875
- w_kup: bfloat16 [512, 1024], P(None, 'tp'), may hold values from -0.25 to 0.25
- w_vup: bfloat16 [512, 1024], P(None, 'tp'), may hold values from -0.25 to 0.25
- qhead_gain: float32 [96], replicated, may hold values from 1.1 to 1.9
- khead_gain: float32 [96], replicated, may hold values from 1.1 to 1.9
- w_out_pool: bfloat16 [1024, 2048], P('tp'), may hold values from -0.1875 to 0.1875
- w_out_attn: bfloat16 [1024, 2048], P('tp'), may hold values from -0.75 to 0.75
Outputs:
- mixed: bfloat16 [24576, 2048], P(('sp', 'tp'))
The draws below stay inside these ranges and needn't reach their ends.
All inputs are finite; a program needn't handle non-finite values.
Results may differ from the reference program's by a relative error of at most 0.025.
Values may be sent and summed in bfloat16 or wider, within the bound.
No kernel may reach another device: no remote copies, remote signals or barrier semaphores. Data moves between devices by JAX's collectives and lax.ppermute only.
A program may use at most 128 MiB of HBM per device.

```python
import math
import jax
import jax.numpy as jnp
from jax import lax

D = 2048
POOL = 1024
GROUP = 256
HEADS = 16
NOPE = 64
ROPE = 32
VDIM = 64
QLAT = 768
KVLAT = 512
TOKENS = 24576
N_TP = 8


def level_of(stream_key, extent, split, low, top_value):
    def one(axis_at, shards_of):
        draws = jax.random.uniform(jax.random.fold_in(jax.random.fold_in(stream_key, 6), axis_at), (shards_of,), jnp.float32, low / len(split), top_value / len(split))
        return jnp.repeat(jnp.exp(draws), extent[axis_at] // shards_of).reshape((-1,) + (1,) * (len(extent) - axis_at - 1))

    level = one(*split[0])
    for cut in split[1:]:
        level = level * one(*cut)
    return level


def noise(own_key, shape, scale, reach, cuts=(), kind=jnp.bfloat16):
    array = jax.random.normal(own_key, shape, jnp.float32) * scale
    if len(cuts) > 0:
        array = level_of(own_key, shape, cuts, -0.22, 0.18) * array
    return jnp.clip(array, min=-reach, max=reach).astype(kind)


def setup_inputs(seed: int = 0) -> dict:
    streams_of = jax.random.split(jax.random.key(seed), 17)
    activations = noise(streams_of[0], (TOKENS, D), 1.0, 6.0, ((0, 256),))
    in_gain = jnp.clip(1.0 + 0.18 * jax.random.normal(streams_of[1], (D,), jnp.float32), 0.1, 1.9)
    w_pool_in = noise(streams_of[2], (D, POOL), D ** -0.5, 0.125, ((1, 8),))
    pool_gain = jnp.clip(1.0 + 0.18 * jax.random.normal(streams_of[3], (POOL,), jnp.float32), 0.1, 1.9)
    w_qlat = noise(streams_of[4], (D, QLAT), D ** -0.5, 0.125, ((1, 8),))
    w_kvlat = noise(streams_of[5], (D, KVLAT), D ** -0.5, 0.125, ((1, 8),))
    w_krope = noise(streams_of[6], (D, ROPE), D ** -0.5, 0.125)
    qlat_gain = jnp.clip(1.0 + 0.18 * jax.random.normal(streams_of[7], (QLAT,), jnp.float32), 0.1, 1.9)
    kvlat_gain = jnp.clip(1.0 + 0.18 * jax.random.normal(streams_of[8], (KVLAT,), jnp.float32), 0.1, 1.9)
    w_qup = noise(streams_of[9], (QLAT, HEADS * (NOPE + ROPE)), QLAT ** -0.5, 0.21875, ((1, 8),))
    w_kup = noise(streams_of[10], (KVLAT, HEADS * NOPE), KVLAT ** -0.5, 0.25, ((1, 8),))
    w_vup = noise(streams_of[11], (KVLAT, HEADS * VDIM), KVLAT ** -0.5, 0.25, ((1, 8),))
    qhead_gain = jnp.clip(jax.random.uniform(streams_of[12], (NOPE + ROPE,), jnp.float32, 1.1, 1.9), 1.1, 1.9)
    khead_gain = jnp.clip(jax.random.uniform(streams_of[13], (NOPE + ROPE,), jnp.float32, 1.1, 1.9), 1.1, 1.9)
    w_out_pool = noise(streams_of[14], (POOL, D), POOL ** -0.5, 0.1875, ((0, 8),))
    w_out_attn = noise(streams_of[15], (HEADS * VDIM, D), (HEADS * VDIM // 16) ** -0.5, 0.75, ((0, 8),))
    return {"activations": activations, "in_gain": in_gain, "w_pool_in": w_pool_in, "pool_gain": pool_gain, "w_qlat": w_qlat, "w_kvlat": w_kvlat, "w_krope": w_krope, "qlat_gain": qlat_gain, "kvlat_gain": kvlat_gain, "w_qup": w_qup, "w_kup": w_kup, "w_vup": w_vup, "qhead_gain": qhead_gain, "khead_gain": khead_gain, "w_out_pool": w_out_pool, "w_out_attn": w_out_attn}


norm_eps = 1e-06
rope_theta = 10000.0
rim_depth = 15
block_rows = 512

def row_norm(source, norm_gain):
    as_float = source.astype(jnp.float32)
    factor = lax.rsqrt(lax.optimization_barrier(jnp.mean(as_float * as_float, axis=-1, keepdims=True)) + norm_eps)
    return as_float * factor * norm_gain

def rotate(head_rows, positions):
    half_rope = ROPE // 2
    frequency = rope_theta ** (-jnp.arange(0, ROPE, 2, dtype=jnp.float32) / ROPE)
    angles = positions.astype(jnp.float32)[:, None] * frequency[None, :]
    cosine = jnp.cos(angles)[:, None, :]
    sine_part = jnp.sin(angles)[:, None, :]
    plain_part = head_rows[..., :NOPE]
    lower_half = head_rows[..., NOPE:NOPE + half_rope]
    upper_half = head_rows[..., NOPE + half_rope:]
    return jnp.concatenate([plain_part, lower_half * cosine - upper_half * sine_part, upper_half * cosine + lower_half * sine_part], axis=-1)

def pool_mix(extended, positions, channel_start):
    row_count = positions.shape[0]
    width = extended.shape[1]
    channel = channel_start + jnp.arange(width, dtype=jnp.int32)
    window = jnp.left_shift(jnp.int32(2), (channel // GROUP).astype(jnp.int32))
    as_float = extended.astype(jnp.float32)
    window_sum = jnp.zeros((row_count, width), jnp.float32)
    for lag_index in range(rim_depth + 1):
        lagged = as_float[rim_depth - lag_index:rim_depth - lag_index + row_count]
        window_sum = window_sum + jnp.where(lag_index < window[None, :], lagged, 0.0)
    divisor = jnp.minimum(positions[:, None] + 1, window[None, :]).astype(jnp.float32)
    return window_sum / divisor - as_float[rim_depth:]

def make_queries(q_normed, w_qup, norm_gain, positions):
    row_count = q_normed.shape[0]
    head_count = w_qup.shape[1] // (NOPE + ROPE)
    query_raw = jnp.dot(q_normed, w_qup, preferred_element_type=jnp.float32).astype(jnp.bfloat16)
    query_raw = query_raw.reshape(row_count, head_count, NOPE + ROPE)
    return rotate(row_norm(query_raw, norm_gain), positions).astype(jnp.bfloat16)

def make_keys(kv_rows, rope_rows, w_kup, w_vup, norm_gain, positions):
    row_count = kv_rows.shape[0]
    head_count = w_kup.shape[1] // NOPE
    key_plain = jnp.dot(kv_rows, w_kup, preferred_element_type=jnp.float32).astype(jnp.bfloat16)
    key_plain = key_plain.reshape(row_count, head_count, NOPE)
    value_rows = jnp.dot(kv_rows, w_vup, preferred_element_type=jnp.float32).astype(jnp.bfloat16)
    shared = jnp.broadcast_to(rope_rows[:, None, :], (row_count, head_count, ROPE))
    joined = jnp.concatenate([key_plain, shared], axis=-1)
    key_rows = rotate(row_norm(joined, norm_gain), positions).astype(jnp.bfloat16)
    return (key_rows.reshape(row_count, head_count * (NOPE + ROPE)), value_rows)

def attend(queries, key_rows, value_rows):
    all_rows, head_count, _ = queries.shape
    block_size = math.gcd(block_rows, all_rows)
    key_rows = key_rows.reshape(all_rows, head_count, NOPE + ROPE)
    value_rows = value_rows.reshape(all_rows, head_count, VDIM)
    score_scale = (NOPE + ROPE) ** (-0.5)

    def one_block(block_index):
        first_row = block_index * block_size
        query_block = lax.dynamic_slice_in_dim(queries, first_row, block_size, 0).astype(jnp.float32)
        query_pos = first_row + jnp.arange(block_size, dtype=jnp.int32)

        def add_keys(key_index, state_pair):
            numerator, denominator = state_pair
            key_first = key_index * block_size
            key_block = lax.dynamic_slice_in_dim(key_rows, key_first, block_size, 0).astype(jnp.float32)
            value_block = lax.dynamic_slice_in_dim(value_rows, key_first, block_size, 0).astype(jnp.float32)
            key_pos = key_first + jnp.arange(block_size, dtype=jnp.int32)
            scores = jnp.einsum('qhd,khd->hqk', query_block, key_block) * score_scale
            weights = jnp.where(key_pos[None, None, :] <= query_pos[None, :, None], jnp.exp(scores), 0.0)
            denominator = denominator + lax.optimization_barrier(jnp.sum(weights, axis=-1))
            rounded = lax.optimization_barrier(weights.astype(jnp.bfloat16)).astype(jnp.float32)
            numerator = numerator + jnp.einsum('hqk,khd->qhd', rounded, value_block)
            return (numerator, denominator)
        start_pair = (jnp.zeros((block_size, head_count, VDIM), jnp.float32), jnp.zeros((head_count, block_size), jnp.float32))
        numerator, denominator = lax.fori_loop(0, block_index + 1, add_keys, start_pair)
        return (numerator / jnp.transpose(denominator)[:, :, None]).astype(jnp.bfloat16)
    blocks_out = lax.map(one_block, jnp.arange(all_rows // block_size, dtype=jnp.int32))
    return blocks_out.reshape(all_rows, head_count * VDIM)

def reference(activations, in_gain, w_pool_in, pool_gain, w_qlat, w_kvlat, w_krope, qlat_gain, kvlat_gain, w_qup, w_kup, w_vup, qhead_gain, khead_gain, w_out_pool, w_out_attn):
    positions = jnp.arange(TOKENS, dtype=jnp.int32)
    normed = row_norm(activations, in_gain).astype(jnp.bfloat16)
    pool_in = jnp.dot(normed, w_pool_in, preferred_element_type=jnp.float32).astype(jnp.bfloat16)
    extended = jnp.concatenate([jnp.zeros((rim_depth, POOL), jnp.bfloat16), pool_in], axis=0)
    pool_out = (pool_mix(extended, positions, 0) * pool_gain).astype(jnp.bfloat16)
    q_latent = jnp.dot(normed, w_qlat, preferred_element_type=jnp.float32).astype(jnp.bfloat16)
    kv_latent = jnp.dot(normed, w_kvlat, preferred_element_type=jnp.float32).astype(jnp.bfloat16)
    rope_key = jnp.dot(normed, w_krope, preferred_element_type=jnp.float32).astype(jnp.bfloat16)
    q_normed = row_norm(q_latent, qlat_gain).astype(jnp.bfloat16)
    kv_normed = row_norm(kv_latent, kvlat_gain).astype(jnp.bfloat16)
    queries = make_queries(q_normed, w_qup, qhead_gain, positions)
    key_rows, value_rows = make_keys(kv_normed, rope_key, w_kup, w_vup, khead_gain, positions)
    attended = attend(queries, key_rows, value_rows)
    pool_span = POOL // N_TP
    attn_span = HEADS * VDIM // N_TP
    mixed = jnp.zeros((TOKENS, D), jnp.float32)
    for block_index in range(N_TP):
        pool_lo = block_index * pool_span
        attn_lo = block_index * attn_span
        partial_value = jnp.dot(pool_out[:, pool_lo:pool_lo + pool_span], w_out_pool[pool_lo:pool_lo + pool_span], preferred_element_type=jnp.float32)
        partial_value = partial_value + jnp.dot(attended[:, attn_lo:attn_lo + attn_span], w_out_attn[attn_lo:attn_lo + attn_span], preferred_element_type=jnp.float32)
        rounded = lax.optimization_barrier(partial_value.astype(jnp.bfloat16)).astype(jnp.float32)
        mixed = mixed + rounded
    return mixed.astype(jnp.bfloat16)
```

```python
import math

import jax
import jax.numpy as jnp
from jax import lax
from jax.experimental import pallas as pl
from jax.experimental.pallas import tpu as pltpu
from jax.sharding import Mesh, PartitionSpec as P

NOPE = 64
ROPE = 32
HEAD = NOPE + ROPE
VDIM = 64
QLAT = 768
KVLAT = 512
NZ, NY, NX, NC = 8, 4, 4, 2
ROWS = 96
OWN = NX * ROWS
BLOCK = OWN * NY
QUERIES = NC * BLOCK
WIDE = NC * OWN
CHUNK = 256
VROWS = VDIM + 16
DEPTH = 128
RIM = 16

norm_eps = 1e-06
rope_theta = 10000.0
bf16 = jnp.bfloat16
f32 = jnp.float32


def shift(x, axis, distance):
    n = lax.axis_size(axis)
    return lax.ppermute(x, axis, [(i, (i + distance) % n) for i in range(n)])


def query_route(k, back=False):
    route = []
    for z in range(NZ):
        for y in range(NY):
            to = (z if y < NY // 2 else NZ - 1 - z) * NY + (y + k) % NY
            route.append((to, z * NY + y) if back else (z * NY + y, to))
    return route


def pick(x, i):
    return lax.dynamic_index_in_dim(x, i, 0, keepdims=False)


def row_norm(source, gain):
    as_float = source.astype(f32)
    factor = lax.rsqrt(jnp.mean(as_float * as_float, axis=-1, keepdims=True) + norm_eps)
    return as_float * factor * gain


def across(w, rows):
    return lax.dot_general(w, rows, (((0,), (1,)), ((), ())), preferred_element_type=f32)


def turned(lower, upper, cosine, sine):
    return lower * cosine - upper * sine, upper * cosine + lower * sine


def attend_kernel(count, first, last, s_ref, own_ref, other_ref, *refs):
    pieces, refs = refs[:count], refs[count:]
    if not first:
        state_ref, refs = refs[0], refs[1:]
    outs, (acc_ref, q_ref, k_ref, v_ref) = refs[:-4], refs[-4:]
    here_z, here_y, core = s_ref[count], s_ref[count + 1], s_ref[count + 2]
    acc_ref[...] = jnp.zeros_like(acc_ref) if first else state_ref[...]
    for g in range(NY):
        for half, ref in enumerate((own_ref, other_ref)):
            q_ref[0:HEAD, g * WIDE + half * OWN : g * WIDE + (half + 1) * OWN] = ref[:, g * OWN : (g + 1) * OWN]
    q_ref[HEAD:DEPTH, :] = jnp.zeros((DEPTH - HEAD, QUERIES), bf16)
    k_ref[:, HEAD:DEPTH] = jnp.zeros((BLOCK, DEPTH - HEAD), bf16)
    v_ref[VDIM:VROWS, :] = jnp.ones((VROWS - VDIM, BLOCK), bf16)

    def strips(u):
        return u + ROWS * sum((u >= ROWS * n).astype(jnp.int32) for n in range(1, NX))

    def key_places(i):
        at = i * CHUNK + lax.broadcasted_iota(jnp.int32, (CHUNK, 1), 0)
        lo, hi = i * CHUNK // OWN, ((i + 1) * CHUNK - 1) // OWN
        place = strips(at - lo * OWN) + WIDE * lax.rem(here_y - lo + NY, NY)
        if hi > lo:
            place = jnp.where(at < hi * OWN, place, strips(at - hi * OWN) + WIDE * lax.rem(here_y - hi + NY, NY))
        return place + core * ROWS

    def add(off, g_y, masked):
        q = q_ref[:, pl.ds(off, WIDE)]
        out = acc_ref[:, pl.ds(off, WIDE)]
        if masked:
            at = lax.broadcasted_iota(jnp.int32, (1, WIDE), 1)
            q_place = jnp.where(at < OWN, strips(at) + core * ROWS, strips(at - OWN) + (1 - core) * ROWS) + WIDE * g_y
        n = BLOCK // CHUNK
        s = jnp.dot(k_ref[0:CHUNK, :], q, preferred_element_type=f32)
        for i in range(n):
            ahead = None
            if i + 1 < n:
                ahead = jnp.dot(k_ref[(i + 1) * CHUNK : (i + 2) * CHUNK, :], q, preferred_element_type=f32)
            weights = jnp.exp2(s)
            if masked:
                weights = jnp.where(key_places(i) <= q_place, weights, 0.0)
            out = out + jnp.dot(v_ref[:, i * CHUNK : (i + 1) * CHUNK], weights.astype(bf16), preferred_element_type=f32)
            s = ahead
        acc_ref[:, pl.ds(off, WIDE)] = out

    def piece_step(b, carry):
        for i, piece in enumerate(pieces):

            @pl.when(b == i)
            def _():
                k_ref[:, 0:HEAD] = piece[0:HEAD, :].T
                v_ref[0:VDIM, :] = piece[HEAD : HEAD + VDIM, :]

        block_z = s_ref[b]

        def group(g, inner):
            g_y = lax.rem(here_y - g + NY, NY)
            g_z = jnp.where(g_y < NY // 2, here_z, NZ - 1 - here_z)
            off = pl.multiple_of(g * WIDE, WIDE)
            pl.when(block_z < g_z)(lambda: add(off, g_y, False))
            pl.when(block_z == g_z)(lambda: add(off, g_y, True))
            return inner

        return lax.fori_loop(0, NY, group, carry)

    lax.fori_loop(0, count, piece_step, 0)
    if last:
        for g in range(NY):
            for half, ref in enumerate(outs):
                ref[:, g * OWN : (g + 1) * OWN] = acc_ref[0 : VDIM + 8, g * WIDE + half * OWN : g * WIDE + (half + 1) * OWN]
    else:
        outs[0][...] = acc_ref[...]


def attend(own, other, pieces, piece_z, place, state, last=False):
    count = len(pieces)
    first = state is None
    whole = pl.BlockSpec(memory_space=pltpu.VMEM)
    scalars = jnp.stack([*piece_z, *place]).astype(jnp.int32)
    operands = [scalars, own, other, *pieces] + ([] if first else [state])
    half = jax.ShapeDtypeStruct((VDIM + 8, BLOCK), f32)
    return pl.pallas_call(
        lambda *refs: attend_kernel(count, first, last, *refs),
        out_shape=(half, half) if last else jax.ShapeDtypeStruct((VROWS, QUERIES), f32),
        in_specs=[pl.BlockSpec(memory_space=pltpu.SMEM)] + [whole] * (len(operands) - 1),
        out_specs=(whole, whole) if last else whole,
        scratch_shapes=[
            pltpu.VMEM((VROWS, QUERIES), f32),
            pltpu.VMEM((DEPTH, QUERIES), bf16),
            pltpu.VMEM((BLOCK, DEPTH), bf16),
            pltpu.VMEM((VROWS, BLOCK), bf16),
        ],
        cost_estimate=pl.CostEstimate(
            flops=4 * count * QUERIES * BLOCK * 256, transcendentals=count * QUERIES * BLOCK, bytes_accessed=4 << 20
        ),
        name="attend",
    )(*operands)


def local(
    activations,
    in_gain,
    w_pool_in,
    pool_gain,
    w_qlat,
    w_kvlat,
    w_krope,
    qlat_gain,
    kvlat_gain,
    w_qup,
    w_kup,
    w_vup,
    qhead_gain,
    khead_gain,
    w_out_pool,
    w_out_attn,
):
    at_z, at_y, at_x, at_c = (lax.axis_index(a) for a in ("z", "y", "x", "c"))

    normed = row_norm(activations, in_gain).astype(bf16)
    arrived = [normed] + [shift(normed, "x", k) for k in range(1, NX)]
    token = jnp.arange(OWN, dtype=jnp.int32)
    positions = (at_z * NY + at_y) * WIDE + (token // ROWS) * (NC * ROWS) + at_c * ROWS + token % ROWS

    narrow = shift(jnp.concatenate([w_kvlat, w_qlat, w_pool_in], axis=1), "c", 1)
    kv_w, q_w = w_kvlat.shape[1], w_qlat.shape[1]
    kv_cut, q_cut = NC * kv_w + ROPE, NC * (kv_w + q_w) + ROPE
    columns = jnp.concatenate(
        [
            w_kvlat, narrow[:, :kv_w], w_krope,
            w_qlat, narrow[:, kv_w : kv_w + q_w],
            w_pool_in, narrow[:, kv_w + q_w :],
        ],
        axis=1,
    )
    projected = jnp.zeros((NX, ROWS, columns.shape[1]), bf16)
    for k, block in enumerate(arrived):
        part = jnp.dot(block, columns, preferred_element_type=f32).astype(bf16)
        projected = lax.dynamic_update_slice(projected, part[None], ((at_x - k) % NX, 0, 0))
    projected = projected.reshape(OWN, -1)

    def in_order(w, width):
        parts = [
            lax.dynamic_slice_in_dim(w, (((at_x - r) % NX) * NC + (at_c + j) % NC) * width, width, 0)
            for r in range(NX)
            for j in range(NC)
        ]
        return jnp.concatenate(parts, axis=0)

    def both(w, axis):
        return jnp.concatenate([w, shift(w, "c", 1)], axis=axis)

    qup = in_order(both(w_qup, 1), q_w)
    kup = in_order(both(w_kup, 1), kv_w)
    vup = in_order(both(w_vup, 1), kv_w)
    q_gain = in_order(qlat_gain, q_w)
    kv_gain = in_order(kvlat_gain, kv_w)

    def slot(m):
        return ((m // 2 + at_c) % NC) * 2 + m % 2

    frequency = rope_theta ** (-jnp.arange(0, ROPE, 2, dtype=f32) / ROPE)
    angles = frequency[:, None] * positions.astype(f32)[None, :]
    cosine, sine = jnp.cos(angles), jnp.sin(angles)

    kv_part = projected[:, : NC * kv_w]
    rope_key = projected[:, NC * kv_w : kv_cut].T.astype(f32)
    kv_latent = jnp.concatenate([kv_part] + [shift(kv_part, "x", k) for k in range(1, NX)], axis=1)
    kv_normed = row_norm(kv_latent, kv_gain).astype(bf16)
    key_plain = across(kup, kv_normed).astype(bf16).reshape(NY, NOPE, OWN).astype(f32)
    value = across(vup, kv_normed).astype(bf16).reshape(NY, VDIM, OWN)
    squares = jnp.sum(key_plain * key_plain, axis=1) + jnp.sum(rope_key * rope_key, axis=0)
    factor = lax.rsqrt(squares / HEAD + norm_eps)[:, None, :]
    k_gain = khead_gain[:, None]
    rope_part = rope_key[None] * factor * k_gain[NOPE:]
    low, high = turned(rope_part[:, : ROPE // 2], rope_part[:, ROPE // 2 :], cosine, sine)
    key_value = jnp.concatenate(
        [(key_plain * factor * k_gain[:NOPE]).astype(bf16), low.astype(bf16), high.astype(bf16), value], axis=1
    )
    piece = jnp.concatenate(
        [pick(key_value, slot(at_y))]
        + [shift(pick(key_value, slot((at_y + k) % NY)), "y", k) for k in range(1, NY)],
        axis=1,
    )

    q_part = projected[:, kv_cut:q_cut]
    q_latent = jnp.concatenate([q_part] + [shift(q_part, "x", k) for k in range(1, NX)], axis=1)
    q_normed = row_norm(q_latent, q_gain).astype(bf16)
    query = across(qup, q_normed).astype(bf16).reshape(NY, HEAD, OWN).astype(f32)
    factor = lax.rsqrt(jnp.mean(query * query, axis=1, keepdims=True) + norm_eps)
    query = query * factor * qhead_gain[:, None] * (HEAD**-0.5 * math.log2(math.e))
    low, high = turned(query[:, NOPE : NOPE + ROPE // 2], query[:, NOPE + ROPE // 2 :], cosine, sine)
    query = jnp.concatenate([query[:, :NOPE], low, high], axis=1).astype(bf16)
    mine = jnp.concatenate(
        [lax.ppermute(pick(query, slot((at_y + k) % NY)), ("z", "y"), query_route(k)) for k in range(NY)], axis=1
    )
    other = shift(mine, "c", 1)

    place = (at_z, at_y, at_c)
    state = attend(mine, other, [piece], [at_z], place, None)
    up, down = piece, piece
    for step in range(1, NZ // 2):
        up, down = shift(up, "z", 1), shift(down, "z", -1)
        state = attend(mine, other, [up, down], [(at_z - step) % NZ, (at_z + step) % NZ], place, state)
    half = BLOCK // 2
    end = jnp.concatenate([shift(up[:, :half], "z", 1), shift(down[:, half:], "z", -1)], axis=1)
    here, there = attend(mine, other, [end], [(at_z + NZ // 2) % NZ], place, state, last=True)

    pool_in = projected[:, q_cut:]
    pool_w = pool_in.shape[1]
    strips = pool_in.reshape(NX, ROWS, pool_w)
    tails = strips[:, ROWS - RIM :]
    other = shift(tails, "c", 1)
    route = [((g - 1) * NC + 1, g * NC) for g in range(1, NZ * NY)]
    far = lax.ppermute(tails[NX - 1], ("z", "y", "c"), route)
    before = jnp.where(at_c == 1, other, jnp.concatenate([far[None], other[: NX - 1]], axis=0))
    before = jnp.concatenate([before[..., pool_w // 2 :], before[..., : pool_w // 2]], axis=-1)
    sums = jnp.concatenate([before, strips], axis=1).astype(f32)
    pooled_sums = []
    for reach in (1, 2, 4, 8):
        sums = sums[:, reach:] + sums[:, :-reach]
        pooled_sums.append(sums[:, sums.shape[1] - ROWS :])
    chosen = pooled_sums[-1]
    for level in range(3):
        chosen = jnp.where(at_x == level, pooled_sums[level], chosen)
    divisor = jnp.minimum(positions + 1, jnp.left_shift(2, at_x)).astype(f32).reshape(NX, ROWS, 1)
    pooled = chosen / divisor - strips.astype(f32)
    pool_out = (pooled * both(pool_gain, 0)).astype(bf16)

    def over_x(blocks):
        parts = [pick(blocks, at_x)] + [shift(pick(blocks, (at_x + k) % NX), "x", k) for k in range(1, NX)]
        return jnp.concatenate(parts, axis=1)

    pool_rows = over_x(pool_out)

    own_w = jnp.concatenate([w_out_pool, w_out_attn], axis=0)
    own_w, mine = lax.optimization_barrier((own_w, mine))
    w1, w3 = shift(own_w, "x", 1), shift(own_w, "x", -1)
    mid = own_w.shape[0] // 2
    w2 = jnp.concatenate([shift(w1[:mid], "x", 1), shift(w3[mid:], "x", -1)], axis=0)
    wide_w = jnp.stack([own_w, w1, w2, w3])
    other_w = shift(wide_w, "c", 1).reshape(2 * NX * own_w.shape[0] // 2, -1)
    wide_w = wide_w.reshape(other_w.shape)

    total = here + shift(there, "c", 1)
    attended = (total[:VDIM] / total[VDIM : VDIM + 1]).astype(bf16)
    home = [
        lax.ppermute(attended[:, k * OWN : (k + 1) * OWN], ("z", "y"), query_route(k, back=True)) for k in range(NY)
    ]
    home = jnp.stack(home)
    order = [pick(home, ((n // 2 + at_c) % NC * 2 + n % 2 - at_y) % NY) for n in range(NY)]
    home = jnp.concatenate(order, axis=0).T.reshape(NX, ROWS, NY * VDIM)
    attn_rows = over_x(home)
    own_rows, other_rows = [], []
    for r in range(NX):
        for source in (pool_rows, attn_rows):
            width = source.shape[1] // NX
            cut = r * width + width // 2
            own_rows.append(source[:, r * width : cut])
            other_rows.append(source[:, cut : (r + 1) * width])
    own_rows, other_rows = jnp.concatenate(own_rows, axis=1), jnp.concatenate(other_rows, axis=1)
    return (
        jnp.dot(own_rows, wide_w, preferred_element_type=f32) + jnp.dot(other_rows, other_w, preferred_element_type=f32)
    ).astype(bf16)


def solution(mesh):
    fine = Mesh(mesh.devices.reshape(NZ, NY, NX, NC), ("z", "y", "x", "c"))
    tp = ("x", "c")
    every = ("z", "y", "x", "c")
    placed = (
        P(every, None),
        P(),
        P(None, tp),
        P(tp),
        P(None, tp),
        P(None, tp),
        P(),
        P(),
        P(),
        P(None, tp),
        P(None, tp),
        P(None, tp),
        P(),
        P(),
        P(tp, None),
        P(tp, None),
    )
    return jax.shard_map(local, mesh=fine, in_specs=placed, out_specs=P(every, None), check_vma=False)
```

```python
import math

import jax
import jax.numpy as jnp
from jax import lax
from jax.experimental import pallas as pl
from jax.experimental.pallas import tpu as pltpu
from jax.sharding import Mesh, PartitionSpec as P

NOPE = 64
ROPE = 32
HEAD = NOPE + ROPE
VDIM = 64
QLAT = 768
KVLAT = 512
NZ, NY, NX, NC = 8, 4, 4, 2
ROWS = 96
OWN = NX * ROWS
BLOCK = OWN * NY
QUERIES = NC * BLOCK
WIDE = NC * OWN
CHUNK = 256
VROWS = VDIM + 16
DEPTH = 128
RIM = 16

norm_eps = 1e-06
rope_theta = 10000.0
bf16 = jnp.bfloat16
f32 = jnp.float32


def shift(x, axis, distance):
    n = lax.axis_size(axis)
    return lax.ppermute(x, axis, [(i, (i + distance) % n) for i in range(n)])


def pick(x, i):
    return lax.dynamic_index_in_dim(x, i, 0, keepdims=False)


def row_norm(source, gain):
    as_float = source.astype(f32)
    factor = lax.rsqrt(jnp.mean(as_float * as_float, axis=-1, keepdims=True) + norm_eps)
    return as_float * factor * gain


def turned(lower, upper, cosine, sine):
    return lower * cosine - upper * sine, upper * cosine + lower * sine


def attend_kernel(steps, first, last, p, own_ref, other_ref, *refs):
    per = 2 if last else 1
    pieces, refs = refs[: per * len(steps)], refs[per * len(steps) :]
    if not first:
        state_ref, refs = refs[0], refs[1:]
    outs, scratch = refs[: 2 if last else 1], refs[2 if last else 1 :]
    acc_ref, q_ref, k_ref, v_ref, half_ref, raw_ref, piece_sem, query_sem, state_sem, out_sem = scratch
    here_z, here_y, core = p[0], p[1], p[3]
    loads = []
    for b in range(len(steps)):
        if last:
            loads.append([pltpu.make_async_copy(pieces[i], raw_ref.at[b, i], piece_sem.at[b, i]) for i in range(2)])
        else:
            loads.append([pltpu.make_async_copy(pieces[b], raw_ref.at[b], piece_sem.at[b, 0])])
    queries = [pltpu.make_async_copy(r, half_ref.at[i], query_sem.at[i]) for i, r in enumerate((own_ref, other_ref))]
    for copy in loads[0] + queries:
        copy.start()
    if not first:
        state_load = pltpu.make_async_copy(state_ref, acc_ref, state_sem)
        state_load.start()
    for more in loads[1:]:
        for copy in more:
            copy.start()
    q_ref[HEAD:DEPTH, :] = jnp.zeros((DEPTH - HEAD, QUERIES), bf16)
    k_ref[:, HEAD:DEPTH] = jnp.zeros((BLOCK, DEPTH - HEAD), bf16)
    v_ref[VDIM:VROWS, :] = jnp.ones((VROWS - VDIM, BLOCK), bf16)
    if first:
        acc_ref[...] = jnp.zeros_like(acc_ref)

    def strips(u):
        return u + ROWS * sum((u >= ROWS * n).astype(jnp.int32) for n in range(1, NX))

    def key_places(i):
        at = i * CHUNK + lax.broadcasted_iota(jnp.int32, (CHUNK, 1), 0)
        lo, hi = i * CHUNK // OWN, ((i + 1) * CHUNK - 1) // OWN
        place = strips(at - lo * OWN) + WIDE * lax.rem(here_y - lo + NY, NY)
        if hi > lo:
            place = jnp.where(at < hi * OWN, place, strips(at - hi * OWN) + WIDE * lax.rem(here_y - hi + NY, NY))
        return place + core * ROWS

    def add(off, g_y, masked):
        q = q_ref[:, pl.ds(off, WIDE)]
        out = acc_ref[:, pl.ds(off, WIDE)]
        if masked:
            at = lax.broadcasted_iota(jnp.int32, (1, WIDE), 1)
            q_place = jnp.where(at < OWN, strips(at) + core * ROWS, strips(at - OWN) + (1 - core) * ROWS) + WIDE * g_y
        n = BLOCK // CHUNK
        s = jnp.dot(k_ref[0:CHUNK, :], q, preferred_element_type=f32)
        for i in range(n):
            ahead = None
            if i + 1 < n:
                ahead = jnp.dot(k_ref[(i + 1) * CHUNK : (i + 2) * CHUNK, :], q, preferred_element_type=f32)
            weights = jnp.exp2(s)
            if masked:
                weights = jnp.where(key_places(i) <= q_place, weights, 0.0)
            out = out + jnp.dot(v_ref[:, i * CHUNK : (i + 1) * CHUNK], weights.astype(bf16), preferred_element_type=f32)
            s = ahead
        acc_ref[:, pl.ds(off, WIDE)] = out

    for b in range(len(steps)):
        for copy in loads[b]:
            copy.wait()
    for copy in queries:
        copy.wait()
    for g in range(NY):
        for half in range(NC):
            q_ref[0:HEAD, g * WIDE + half * OWN : g * WIDE + (half + 1) * OWN] = half_ref[half, :, g * OWN : (g + 1) * OWN]
    if not first:
        state_load.wait()

    def piece_step(b, carry):
        step = steps[0] if len(steps) == 1 else jnp.where(b == 0, steps[0], steps[1])
        block_z = lax.rem(here_z + step + NZ, NZ)

        def compute():
            for i in range(2):
                cut = BLOCK // 2
                k_ref[i * cut : (i + 1) * cut, 0:HEAD] = raw_ref[b, i, 0:HEAD, :].T
                v_ref[0:VDIM, i * cut : (i + 1) * cut] = raw_ref[b, i, HEAD : HEAD + VDIM, :]

            def group(g, inner):
                add(pl.multiple_of(g * WIDE, WIDE), lax.rem(here_y - g + NY, NY), first)
                return inner

            lax.fori_loop(0, NY, group, 0)

        if first:
            compute()
        else:
            pl.when(block_z < here_z)(compute)
        return carry

    lax.fori_loop(0, len(steps), piece_step, 0)
    stores = []
    if last:
        for g in range(NY):
            for half, ref in enumerate(outs):
                source = acc_ref.at[0 : VDIM + 8, g * WIDE + half * OWN : g * WIDE + (half + 1) * OWN]
                target = ref.at[:, g * OWN : (g + 1) * OWN]
                stores.append(pltpu.make_async_copy(source, target, out_sem.at[g, half]))
    else:
        for g in range(NY):
            cut = slice(g * WIDE, (g + 1) * WIDE)
            stores.append(pltpu.make_async_copy(acc_ref.at[:, cut], outs[0].at[:, cut], out_sem.at[g, 0]))
    for copy in stores:
        copy.start()
    for copy in stores:
        copy.wait()


def attend(own, other, pieces, steps, place, state, last=False):
    first = state is None
    anywhere = pl.BlockSpec(memory_space=pl.ANY)
    operands = [place, own, other, *pieces] + ([] if first else [state])
    half = jax.ShapeDtypeStruct((VDIM + 8, BLOCK), f32)
    count = len(steps)
    return pl.pallas_call(
        lambda *refs: attend_kernel(steps, first, last, *refs),
        out_shape=(half, half) if last else jax.ShapeDtypeStruct((VROWS, QUERIES), f32),
        in_specs=[pl.BlockSpec(memory_space=pltpu.SMEM)] + [anywhere] * (len(operands) - 1),
        out_specs=(anywhere, anywhere) if last else anywhere,
        scratch_shapes=[
            pltpu.VMEM((VROWS, QUERIES), f32),
            pltpu.VMEM((DEPTH, QUERIES), bf16),
            pltpu.VMEM((BLOCK, DEPTH), bf16),
            pltpu.VMEM((VROWS, BLOCK), bf16),
            pltpu.VMEM((NC, HEAD, BLOCK), bf16),
            pltpu.VMEM((count, 2, HEAD + VDIM, BLOCK // 2), bf16),
            pltpu.SemaphoreType.DMA((count, 2)),
            pltpu.SemaphoreType.DMA((NC,)),
            pltpu.SemaphoreType.DMA,
            pltpu.SemaphoreType.DMA((NY, NC)),
        ],
        cost_estimate=pl.CostEstimate(
            flops=4 * count * QUERIES * BLOCK * 256, transcendentals=count * QUERIES * BLOCK, bytes_accessed=4 << 20
        ),
        name="attend",
    )(*operands)


WHOLE = pl.BlockSpec(memory_space=pltpu.VMEM)
SCALARS = pl.BlockSpec(memory_space=pltpu.SMEM)
HALVES = [pl.BlockSpec((128, 2048), lambda i, h=h: (h, 0)) for h in range(2)]
KEY_WIDTH = NC * KVLAT // (NX * NC)
QUERY_WIDTH = NC * QLAT // (NX * NC)


def on_chip(kernel, outs, place, *operands, scratch=(), flops=1 << 30, specs=None):
    return pl.pallas_call(
        kernel,
        out_shape=outs,
        grid=(1,) if specs else (),
        in_specs=[SCALARS] + (specs or [WHOLE] * len(operands)),
        out_specs=jax.tree.map(lambda _: WHOLE, outs),
        scratch_shapes=list(scratch),
        cost_estimate=pl.CostEstimate(flops=flops, transcendentals=0, bytes_accessed=4 << 20),
    )(place, *operands)


def struct(*shape, dtype=bf16):
    return jax.ShapeDtypeStruct(shape, dtype)


def mod(i, n):
    return lax.rem(i + n, n)


def arrange_kernel(p, kv, kv_o, q, q_o, rope, kup, kup_o, vup, vup_o, qup, qup_o, down_ref, kv_ref, q_ref):
    core = p[3]
    width = KEY_WIDTH // NC
    for i, (mine, there) in enumerate(((kv, q), (kv_o, q_o))):
        c = mod(core + i, NC)
        down_ref[pl.ds(pl.multiple_of(c * width, width), width), :] = mine[...].T
        wide = QUERY_WIDTH // NC
        down_ref[pl.ds(pl.multiple_of(KEY_WIDTH + ROPE + c * wide, ROPE), wide), :] = there[...].T
    down_ref[KEY_WIDTH : KEY_WIDTH + ROPE, :] = rope[...].T
    for i, (k, v, w) in enumerate(((kup, vup, qup), (kup_o, vup_o, qup_o))):
        c = mod(core + i, NC)
        k, v, w = k[...].T, v[...].T, w[...].T
        for h in range(2):
            m = c * 2 + h
            both = NOPE + VDIM
            kv_ref[pl.ds(pl.multiple_of(m * both, both), NOPE), :] = k[h * NOPE : (h + 1) * NOPE]
            kv_ref[pl.ds(pl.multiple_of(m * both + NOPE, NOPE), VDIM), :] = v[h * VDIM : (h + 1) * VDIM]
            q_ref[pl.ds(pl.multiple_of(m * HEAD, ROPE), HEAD), :] = w[h * HEAD : (h + 1) * HEAD]


def project_kernel(p, b0, b1, b2, b3, w, rows_ref, kv_ref, rope_ref, q_ref):
    x = p[2]
    for k, block in enumerate((b0, b1, b2, b3)):
        at = pl.multiple_of(mod(x - k, NX) * ROWS, ROPE)
        rows_ref[pl.ds(at, ROWS), :] = block[...]
    out = lax.dot_general(w[...], rows_ref[...], (((1,), (1,)), ((), ())), preferred_element_type=f32).astype(bf16)
    kv_ref[...] = out[:KEY_WIDTH]
    rope_ref[...] = out[KEY_WIDTH : KEY_WIDTH + ROPE]
    q_ref[...] = out[KEY_WIDTH + ROPE :]


def column(row_ref):
    return jnp.broadcast_to(row_ref[...], (8, row_ref.shape[1])).T[:, 0:1]


def latent_rows(p, parts, lat_ref, gain):
    x = p[2]
    width = parts[0].shape[0]
    for r, part in enumerate(parts):
        lat_ref[pl.ds(pl.multiple_of(mod(x - r, NX) * width, 64), width), :] = part[...].astype(f32)
    lat = lat_ref[...]
    factor = lax.rsqrt(jnp.mean(lat * lat, axis=0, keepdims=True) + norm_eps)
    return (lat * factor * column(gain)).astype(bf16)


def key_kernel(p, p0, p1, p2, p3, rope_ref, w, gain, head_gain, cos, sin, o0, o1, o2, o3, lat_ref, up_ref):
    normed = latent_rows(p, (p0, p1, p2, p3), lat_ref, gain)
    up_ref[...] = jnp.dot(w[...], normed, preferred_element_type=f32).astype(bf16).astype(f32)
    head_gain = column(head_gain)
    rope = rope_ref[...].astype(f32)
    rope_squares = jnp.sum(rope * rope, axis=0, keepdims=True)
    both = NOPE + VDIM
    for k, out in enumerate((o0, o1, o2, o3)):
        m = mod(p[1] + k, NY)
        plain = up_ref[pl.ds(pl.multiple_of(m * both, both), NOPE), :]
        factor = lax.rsqrt((jnp.sum(plain * plain, axis=0, keepdims=True) + rope_squares) / HEAD + norm_eps)
        out[0:NOPE, :] = (plain * factor * head_gain[0:NOPE]).astype(bf16)
        part = rope * factor * head_gain[NOPE:HEAD]
        low, high = turned(part[: ROPE // 2], part[ROPE // 2 :], cos[...], sin[...])
        out[NOPE : NOPE + ROPE // 2, :] = low.astype(bf16)
        out[NOPE + ROPE // 2 : HEAD, :] = high.astype(bf16)
        out[HEAD:, :] = up_ref[pl.ds(pl.multiple_of(m * both + NOPE, NOPE), VDIM), :].astype(bf16)


def query_kernel(p, p0, p1, p2, p3, w, gain, head_gain, cos, sin, o0, o1, o2, o3, lat_ref, up_ref):
    normed = latent_rows(p, (p0, p1, p2, p3), lat_ref, gain)
    up_ref[...] = jnp.dot(w[...], normed, preferred_element_type=f32).astype(bf16).astype(f32)
    scale = column(head_gain) * (HEAD**-0.5 * math.log2(math.e))
    for k, out in enumerate((o0, o1, o2, o3)):
        m = mod(p[1] + k, NY)
        raw = up_ref[pl.ds(pl.multiple_of(m * HEAD, ROPE), HEAD), :]
        factor = lax.rsqrt(jnp.mean(raw * raw, axis=0, keepdims=True) + norm_eps)
        part = raw * factor * scale
        low, high = turned(part[NOPE : NOPE + ROPE // 2], part[NOPE + ROPE // 2 :], cos[...], sin[...])
        out[0:NOPE, :] = part[:NOPE].astype(bf16)
        out[NOPE : NOPE + ROPE // 2, :] = low.astype(bf16)
        out[NOPE + ROPE // 2 :, :] = high.astype(bf16)


def merge_kernel(p, here, there, out):
    total = here[...] + there[...]
    result = (total[:VDIM] / total[VDIM : VDIM + 1]).astype(bf16)
    for k in range(NY):
        y = mod(p[1] - k, NY)
        for x in range(NX):
            out[y * NX + x] = result[:, k * OWN + x * ROWS : k * OWN + (x + 1) * ROWS]


def output_kernel(attn, p, *refs):
    rows, refs = (refs[:1], refs[1:]) if attn else (refs[:NX], refs[NX:])
    weights, refs = refs[: NC * NX], refs[NC * NX :]
    out = refs[-1]
    half = weights[0].shape[0]
    total = refs[0][...] if attn else jnp.zeros(out.shape, f32)
    for i in range(NC):
        for r in range(NX):
            if attn:
                head = mod(p[3] + i, NC) * 2
                pair = [rows[0][(head + h) * NX + mod(p[2] - r, NX)] for h in range(2)]
                part = jnp.concatenate(pair, axis=0).T
            else:
                part = rows[r][:, i * half : (i + 1) * half]
            total = total + jnp.dot(part, weights[i * NX + r][...], preferred_element_type=f32)
    out[...] = total.astype(out.dtype)


def local(
    activations,
    in_gain,
    w_pool_in,
    pool_gain,
    w_qlat,
    w_kvlat,
    w_krope,
    qlat_gain,
    kvlat_gain,
    w_qup,
    w_kup,
    w_vup,
    qhead_gain,
    khead_gain,
    w_out_pool,
    w_out_attn,
):
    at_z, at_y, at_x, at_c = (lax.axis_index(a) for a in ("z", "y", "x", "c"))
    place = jnp.stack([at_z, at_y, at_x, at_c]).astype(jnp.int32)

    normed = row_norm(activations, in_gain).astype(bf16)
    arrived = [normed] + [shift(normed, "x", k) for k in range(1, NX)]
    (normed, w_kvlat, w_qlat, w_kup, w_vup, w_qup) = lax.optimization_barrier(
        (normed, w_kvlat, w_qlat, w_kup, w_vup, w_qup)
    )
    token = jnp.arange(OWN, dtype=jnp.int32)
    positions = (at_z * NY + at_y) * WIDE + (token // ROWS) * (NC * ROWS) + at_c * ROWS + token % ROWS

    def beside(w):
        return w, shift(w, "c", 1)

    down, kv_up, q_up = on_chip(
        arrange_kernel,
        (
            struct(KEY_WIDTH + ROPE + QUERY_WIDTH, activations.shape[1]),
            struct(NY * (NOPE + VDIM), KVLAT),
            struct(NY * HEAD, QLAT),
        ),
        place, *beside(w_kvlat), *beside(w_qlat), w_krope, *beside(w_kup), *beside(w_vup), *beside(w_qup),
    )
    frequency = rope_theta ** (-jnp.arange(0, ROPE, 2, dtype=f32) / ROPE)
    angles = frequency[:, None] * positions.astype(f32)[None, :]
    cosine, sine = jnp.cos(angles), jnp.sin(angles)
    kv_gain, q_gain, k_gain, qh_gain = (g[None] for g in (kvlat_gain, qlat_gain, khead_gain, qhead_gain))
    down, cosine, sine, kv_gain, q_gain, k_gain, qh_gain = lax.optimization_barrier(
        (down, cosine, sine, kv_gain, q_gain, k_gain, qh_gain)
    )

    rows, kv_part, rope_key, q_part = on_chip(
        project_kernel,
        (
            struct(OWN, activations.shape[1]),
            struct(KEY_WIDTH, OWN),
            struct(ROPE, OWN),
            struct(QUERY_WIDTH, OWN),
        ),
        place, *arrived, down,
    )

    kv_parts = [kv_part] + [shift(kv_part, "x", k) for k in range(1, NX)]
    key_values = on_chip(
        key_kernel,
        (struct(HEAD + VDIM, OWN),) * NY,
        place, *kv_parts, rope_key, kv_up, kv_gain, k_gain, cosine, sine,
        scratch=(pltpu.VMEM((KVLAT, OWN), f32), pltpu.VMEM((NY * (NOPE + VDIM), OWN), f32)),
    )
    slots = [key_values[0]] + [shift(key_values[k], "y", k) for k in range(1, NY)]
    piece = jnp.stack([jnp.concatenate(slots[:2], axis=1), jnp.concatenate(slots[2:], axis=1)])
    piece, rows = lax.optimization_barrier((piece, rows))

    q_parts = [q_part] + [shift(q_part, "x", k) for k in range(1, NX)]
    queries = on_chip(
        query_kernel,
        (struct(HEAD, OWN),) * NY,
        place, *q_parts, q_up, q_gain, qh_gain, cosine, sine,
        scratch=(pltpu.VMEM((QLAT, OWN), f32), pltpu.VMEM((NY * HEAD, OWN), f32)),
    )
    own_w = jnp.concatenate([w_out_pool, w_out_attn], axis=0)
    weights = [own_w] + [shift(own_w, "x", k) for k in range(1, NX)]
    mine = jnp.concatenate([queries[0]] + [shift(queries[k], "y", k) for k in range(1, NY)], axis=1)
    other = shift(mine, "c", 1)

    pool_cols = jnp.concatenate(beside(w_pool_in), axis=1)
    pool_in = jnp.dot(rows, pool_cols, preferred_element_type=f32).astype(bf16)
    pool_w = pool_in.shape[1]
    strips = pool_in.reshape(NX, ROWS, pool_w)
    tails = strips[:, ROWS - RIM :]
    across = shift(tails, "c", 1)
    route = [((g - 1) * NC + 1, g * NC) for g in range(1, NZ * NY)]
    far = lax.ppermute(tails[NX - 1], ("z", "y", "c"), route)
    across = jnp.concatenate([across[..., pool_w // 2 :], across[..., : pool_w // 2]], axis=-1)
    far = jnp.concatenate([far[..., pool_w // 2 :], far[..., : pool_w // 2]], axis=-1)
    before = jnp.where(at_c == 1, across, jnp.concatenate([far[None], across[: NX - 1]], axis=0))
    sums = jnp.concatenate([before, strips], axis=1).astype(f32)
    pooled_sums = []
    for reach in (1, 2, 4, 8):
        sums = sums[:, reach:] + sums[:, :-reach]
        pooled_sums.append(sums[:, sums.shape[1] - ROWS :])
    chosen = pooled_sums[-1]
    for level in range(3):
        chosen = jnp.where(at_x == level, pooled_sums[level], chosen)
    divisor = jnp.minimum(positions + 1, jnp.left_shift(2, at_x)).astype(f32).reshape(NX, ROWS, 1)
    pooled = chosen / divisor - strips.astype(f32)
    pool_out = (pooled * jnp.concatenate(beside(pool_gain))).astype(bf16)
    pool_rows = [pick(pool_out, at_x)] + [shift(pick(pool_out, (at_x + k) % NX), "x", k) for k in range(1, NX)]
    state = attend(mine, other, [piece], (0,), place, None)
    up, down = piece, piece
    for step in range(1, NZ // 2):
        up, down = shift(up, "z", 1), shift(down, "z", -1)
        if step == 3:
            state, *weights = lax.optimization_barrier((state, *weights))
            pool_rows = list(pool_rows)
            weights += [shift(w, "c", 1) for w in weights]
        state = attend(mine, other, [up, down], (-step, step), place, state)
    end = [shift(up[0], "z", 1), shift(down[1], "z", -1)]
    pool_term = on_chip(
        lambda *refs: output_kernel(False, *refs),
        struct(ROWS, activations.shape[1], dtype=f32),
        place, *pool_rows, *weights,
        specs=[WHOLE] * NX + [HALVES[0]] * (NC * NX),
    )
    state, pool_term, *weights = lax.optimization_barrier((state, pool_term, *weights))
    here, there = attend(mine, other, end, (NZ // 2,), place, state, last=True)

    attended = on_chip(merge_kernel, struct(NY * NX, VDIM, ROWS), place, here, shift(there, "c", 1))
    attn_rows = lax.all_to_all(attended, ("y", "x"), 0, 0, tiled=True)
    return on_chip(
        lambda *refs: output_kernel(True, *refs),
        struct(ROWS, activations.shape[1]),
        place, attn_rows, *weights, pool_term,
        specs=[WHOLE] + [HALVES[1]] * (NC * NX) + [WHOLE],
    )


def solution(mesh):
    fine = Mesh(mesh.devices.reshape(NZ, NY, NX, NC), ("z", "y", "x", "c"))
    tp = ("x", "c")
    every = ("z", "y", "x", "c")
    placed = (
        P(every, None),
        P(),
        P(None, tp),
        P(tp),
        P(None, tp),
        P(None, tp),
        P(),
        P(),
        P(),
        P(None, tp),
        P(None, tp),
        P(None, tp),
        P(),
        P(),
        P(tp, None),
        P(tp, None),
    )

    return jax.shard_map(local, mesh=fine, in_specs=placed, out_specs=P(every, None), check_vma=False)
```

```python
import math

import jax
import jax.numpy as jnp
from jax import lax
from jax.experimental import pallas as pl
from jax.experimental.pallas import tpu as pltpu
from jax.sharding import Mesh, PartitionSpec as P

NOPE = 64
ROPE = 32
HEAD = NOPE + ROPE
VDIM = 64
QLAT = 768
KVLAT = 512
NZ, NY, NX, NC = 8, 4, 4, 2
ROWS = 96
OWN = NX * ROWS
BLOCK = OWN * NY
QUERIES = NC * BLOCK
WIDE = NC * OWN
CHUNK = 256
VROWS = VDIM + 16
DEPTH = 128
RIM = 16

norm_eps = 1e-06
rope_theta = 10000.0
bf16 = jnp.bfloat16
f32 = jnp.float32


def shift(x, axis, distance):
    n = lax.axis_size(axis)
    return lax.ppermute(x, axis, [(i, (i + distance) % n) for i in range(n)])


def pick(x, i):
    return lax.dynamic_index_in_dim(x, i, 0, keepdims=False)


def row_norm(source, gain):
    as_float = source.astype(f32)
    factor = lax.rsqrt(jnp.mean(as_float * as_float, axis=-1, keepdims=True) + norm_eps)
    return as_float * factor * gain


def turned(lower, upper, cosine, sine):
    return lower * cosine - upper * sine, upper * cosine + lower * sine


def attend_kernel(steps, first, last, p, own_ref, other_ref, *refs):
    pieces, refs = refs[: len(steps)], refs[len(steps) :]
    if not first:
        state_ref, refs = refs[0], refs[1:]
    outs, scratch = refs[: 2 if last else 1], refs[2 if last else 1 :]
    acc_ref, q_ref, k_ref, v_ref, half_ref, raw_ref, piece_sem, query_sem, state_sem, out_sem = scratch
    here_z, here_y, core = p[0], p[1], p[3]
    loads = [pltpu.make_async_copy(piece, raw_ref.at[b], piece_sem.at[b]) for b, piece in enumerate(pieces)]
    queries = [pltpu.make_async_copy(r, half_ref.at[i], query_sem.at[i]) for i, r in enumerate((own_ref, other_ref))]
    for copy in loads[:1] + queries:
        copy.start()
    if not first:
        state_load = pltpu.make_async_copy(state_ref, acc_ref, state_sem)
        state_load.start()
    for copy in loads[1:]:
        copy.start()
    q_ref[HEAD:DEPTH, :] = jnp.zeros((DEPTH - HEAD, QUERIES), bf16)
    k_ref[:, HEAD:DEPTH] = jnp.zeros((BLOCK, DEPTH - HEAD), bf16)
    v_ref[VDIM:VROWS, :] = jnp.ones((VROWS - VDIM, BLOCK), bf16)
    if first:
        acc_ref[...] = jnp.zeros_like(acc_ref)

    def strips(u):
        return u + ROWS * sum((u >= ROWS * n).astype(jnp.int32) for n in range(1, NX))

    def key_places(i):
        at = i * CHUNK + lax.broadcasted_iota(jnp.int32, (CHUNK, 1), 0)
        lo, hi = i * CHUNK // OWN, ((i + 1) * CHUNK - 1) // OWN
        place = strips(at - lo * OWN) + WIDE * lax.rem(here_y - lo + NY, NY)
        if hi > lo:
            place = jnp.where(at < hi * OWN, place, strips(at - hi * OWN) + WIDE * lax.rem(here_y - hi + NY, NY))
        return place + core * ROWS

    def add(off, g_y, masked):
        q = q_ref[:, pl.ds(off, WIDE)]
        out = acc_ref[:, pl.ds(off, WIDE)]
        if masked:
            at = lax.broadcasted_iota(jnp.int32, (1, WIDE), 1)
            q_place = jnp.where(at < OWN, strips(at) + core * ROWS, strips(at - OWN) + (1 - core) * ROWS) + WIDE * g_y
        n = BLOCK // CHUNK
        s = jnp.dot(k_ref[0:CHUNK, :], q, preferred_element_type=f32)
        for i in range(n):
            ahead = None
            if i + 1 < n:
                ahead = jnp.dot(k_ref[(i + 1) * CHUNK : (i + 2) * CHUNK, :], q, preferred_element_type=f32)
            weights = jnp.exp2(s)
            if masked:
                weights = jnp.where(key_places(i) <= q_place, weights, 0.0)
            out = out + jnp.dot(v_ref[:, i * CHUNK : (i + 1) * CHUNK], weights.astype(bf16), preferred_element_type=f32)
            s = ahead
        acc_ref[:, pl.ds(off, WIDE)] = out

    for copy in loads:
        copy.wait()
    for copy in queries:
        copy.wait()
    for g in range(NY):
        for half in range(NC):
            q_ref[0:HEAD, g * WIDE + half * OWN : g * WIDE + (half + 1) * OWN] = half_ref[half, :, g * OWN : (g + 1) * OWN]
    if not first:
        state_load.wait()

    def piece_add(b, masked):
        for i in range(2):
            cut = BLOCK // 2
            k_ref[i * cut : (i + 1) * cut, 0:HEAD] = raw_ref[b, i, 0:HEAD, :].T
            v_ref[0:VDIM, i * cut : (i + 1) * cut] = raw_ref[b, i, HEAD : HEAD + VDIM, :]

        def group(g, inner):
            add(pl.multiple_of(g * WIDE, WIDE), lax.rem(here_y - g + NY, NY), masked)
            return inner

        lax.fori_loop(0, NY, group, 0)

    def piece_step(b, carry):
        step = jnp.int32(steps[-1])
        for i in range(len(steps) - 1):
            step = jnp.where(b == i, steps[i], step)
        pl.when(lax.rem(here_z + step + NZ, NZ) < here_z)(lambda: piece_add(b, False))
        return carry

    if first:
        piece_add(0, True)
    lax.fori_loop(int(first), len(steps), piece_step, 0)
    stores = []
    if last:
        for g in range(NY):
            for half, ref in enumerate(outs):
                source = acc_ref.at[0 : VDIM + 8, g * WIDE + half * OWN : g * WIDE + (half + 1) * OWN]
                target = ref.at[:, g * OWN : (g + 1) * OWN]
                stores.append(pltpu.make_async_copy(source, target, out_sem.at[g, half]))
    else:
        for g in range(NY):
            cut = slice(g * WIDE, (g + 1) * WIDE)
            stores.append(pltpu.make_async_copy(acc_ref.at[:, cut], outs[0].at[:, cut], out_sem.at[g, 0]))
    for copy in stores:
        copy.start()
    for copy in stores:
        copy.wait()


def attend(own, other, pieces, steps, place, state, last=False):
    first = state is None
    anywhere = pl.BlockSpec(memory_space=pl.ANY)
    operands = [place, own, other, *pieces] + ([] if first else [state])
    half = jax.ShapeDtypeStruct((VDIM + 8, BLOCK), f32)
    count = len(steps)
    return pl.pallas_call(
        lambda *refs: attend_kernel(steps, first, last, *refs),
        out_shape=(half, half) if last else jax.ShapeDtypeStruct((VROWS, QUERIES), f32),
        in_specs=[pl.BlockSpec(memory_space=pltpu.SMEM)] + [anywhere] * (len(operands) - 1),
        out_specs=(anywhere, anywhere) if last else anywhere,
        scratch_shapes=[
            pltpu.VMEM((VROWS, QUERIES), f32),
            pltpu.VMEM((DEPTH, QUERIES), bf16),
            pltpu.VMEM((BLOCK, DEPTH), bf16),
            pltpu.VMEM((VROWS, BLOCK), bf16),
            pltpu.VMEM((NC, HEAD, BLOCK), bf16),
            pltpu.VMEM((count, 2, HEAD + VDIM, BLOCK // 2), bf16),
            pltpu.SemaphoreType.DMA((count,)),
            pltpu.SemaphoreType.DMA((NC,)),
            pltpu.SemaphoreType.DMA,
            pltpu.SemaphoreType.DMA((NY, NC)),
        ],
        cost_estimate=pl.CostEstimate(
            flops=4 * count * QUERIES * BLOCK * 256, transcendentals=count * QUERIES * BLOCK, bytes_accessed=4 << 20
        ),
        name="attend",
    )(*operands)


WHOLE = pl.BlockSpec(memory_space=pltpu.VMEM)
SCALARS = pl.BlockSpec(memory_space=pltpu.SMEM)
HALVES = [pl.BlockSpec((128, 2048), lambda i, h=h: (h, 0)) for h in range(2)]
KEY_WIDTH = NC * KVLAT // (NX * NC)
QUERY_WIDTH = NC * QLAT // (NX * NC)


def on_chip(kernel, outs, place, *operands, scratch=(), flops=1 << 30, specs=None):
    return pl.pallas_call(
        kernel,
        out_shape=outs,
        grid=(1,) if specs else (),
        in_specs=[SCALARS] + (specs or [WHOLE] * len(operands)),
        out_specs=jax.tree.map(lambda _: WHOLE, outs),
        scratch_shapes=list(scratch),
        cost_estimate=pl.CostEstimate(flops=flops, transcendentals=0, bytes_accessed=4 << 20),
    )(place, *operands)


def struct(*shape, dtype=bf16):
    return jax.ShapeDtypeStruct(shape, dtype)


def mod(i, n):
    return lax.rem(i + n, n)


def arrange_kernel(p, kv, kv_o, q, q_o, rope, kup, kup_o, vup, vup_o, qup, qup_o, down_ref, kv_ref, q_ref):
    core = p[3]
    width = KEY_WIDTH // NC
    for i, (mine, there) in enumerate(((kv, q), (kv_o, q_o))):
        c = mod(core + i, NC)
        down_ref[pl.ds(pl.multiple_of(c * width, width), width), :] = mine[...].T
        wide = QUERY_WIDTH // NC
        down_ref[pl.ds(pl.multiple_of(KEY_WIDTH + ROPE + c * wide, ROPE), wide), :] = there[...].T
    down_ref[KEY_WIDTH : KEY_WIDTH + ROPE, :] = rope[...].T
    for i, (k, v, w) in enumerate(((kup, vup, qup), (kup_o, vup_o, qup_o))):
        c = mod(core + i, NC)
        k, v, w = k[...].T, v[...].T, w[...].T
        for h in range(2):
            m = c * 2 + h
            both = NOPE + VDIM
            kv_ref[pl.ds(pl.multiple_of(m * both, both), NOPE), :] = k[h * NOPE : (h + 1) * NOPE]
            kv_ref[pl.ds(pl.multiple_of(m * both + NOPE, NOPE), VDIM), :] = v[h * VDIM : (h + 1) * VDIM]
            q_ref[pl.ds(pl.multiple_of(m * HEAD, ROPE), HEAD), :] = w[h * HEAD : (h + 1) * HEAD]


def project_kernel(p, b0, b1, b2, b3, w, rows_ref, kv_ref, rope_ref, q_ref):
    x = p[2]
    for k, block in enumerate((b0, b1, b2, b3)):
        at = pl.multiple_of(mod(x - k, NX) * ROWS, ROPE)
        rows_ref[pl.ds(at, ROWS), :] = block[...]
    out = lax.dot_general(w[...], rows_ref[...], (((1,), (1,)), ((), ())), preferred_element_type=f32).astype(bf16)
    kv_ref[...] = out[:KEY_WIDTH]
    rope_ref[...] = out[KEY_WIDTH : KEY_WIDTH + ROPE]
    q_ref[...] = out[KEY_WIDTH + ROPE :]


def column(row_ref):
    return jnp.broadcast_to(row_ref[...], (8, row_ref.shape[1])).T[:, 0:1]


def latent_rows(p, parts, lat_ref, gain):
    x = p[2]
    width = parts[0].shape[0]
    for r, part in enumerate(parts):
        lat_ref[pl.ds(pl.multiple_of(mod(x - r, NX) * width, 64), width), :] = part[...].astype(f32)
    lat = lat_ref[...]
    factor = lax.rsqrt(jnp.mean(lat * lat, axis=0, keepdims=True) + norm_eps)
    return (lat * factor * column(gain)).astype(bf16)


def key_kernel(p, p0, p1, p2, p3, rope_ref, w, gain, head_gain, cos, sin, o0, o1, o2, o3, lat_ref, up_ref):
    normed = latent_rows(p, (p0, p1, p2, p3), lat_ref, gain)
    up_ref[...] = jnp.dot(w[...], normed, preferred_element_type=f32).astype(bf16).astype(f32)
    head_gain = column(head_gain)
    rope = rope_ref[...].astype(f32)
    rope_squares = jnp.sum(rope * rope, axis=0, keepdims=True)
    both = NOPE + VDIM
    for k, out in enumerate((o0, o1, o2, o3)):
        m = mod(p[1] + k, NY)
        plain = up_ref[pl.ds(pl.multiple_of(m * both, both), NOPE), :]
        factor = lax.rsqrt((jnp.sum(plain * plain, axis=0, keepdims=True) + rope_squares) / HEAD + norm_eps)
        out[0:NOPE, :] = (plain * factor * head_gain[0:NOPE]).astype(bf16)
        part = rope * factor * head_gain[NOPE:HEAD]
        low, high = turned(part[: ROPE // 2], part[ROPE // 2 :], cos[...], sin[...])
        out[NOPE : NOPE + ROPE // 2, :] = low.astype(bf16)
        out[NOPE + ROPE // 2 : HEAD, :] = high.astype(bf16)
        out[HEAD:, :] = up_ref[pl.ds(pl.multiple_of(m * both + NOPE, NOPE), VDIM), :].astype(bf16)


def query_kernel(p, p0, p1, p2, p3, w, gain, head_gain, cos, sin, o0, o1, o2, o3, lat_ref, up_ref):
    normed = latent_rows(p, (p0, p1, p2, p3), lat_ref, gain)
    up_ref[...] = jnp.dot(w[...], normed, preferred_element_type=f32).astype(bf16).astype(f32)
    scale = column(head_gain) * (HEAD**-0.5 * math.log2(math.e))
    for k, out in enumerate((o0, o1, o2, o3)):
        m = mod(p[1] + k, NY)
        raw = up_ref[pl.ds(pl.multiple_of(m * HEAD, ROPE), HEAD), :]
        factor = lax.rsqrt(jnp.mean(raw * raw, axis=0, keepdims=True) + norm_eps)
        part = raw * factor * scale
        low, high = turned(part[NOPE : NOPE + ROPE // 2], part[NOPE + ROPE // 2 :], cos[...], sin[...])
        out[0:NOPE, :] = part[:NOPE].astype(bf16)
        out[NOPE : NOPE + ROPE // 2, :] = low.astype(bf16)
        out[NOPE + ROPE // 2 :, :] = high.astype(bf16)


def merge_kernel(p, here, there, out):
    total = here[...] + there[...]
    result = (total[:VDIM] / total[VDIM : VDIM + 1]).astype(bf16)
    for k in range(NY):
        y = mod(p[1] - k, NY)
        for x in range(NX):
            out[y * NX + x] = result[:, k * OWN + x * ROWS : k * OWN + (x + 1) * ROWS]


def output_kernel(attn, p, *refs):
    rows, refs = (refs[:1], refs[1:]) if attn else (refs[:NX], refs[NX:])
    weights, refs = refs[: NC * NX], refs[NC * NX :]
    out = refs[-1]
    half = weights[0].shape[0]
    total = refs[0][...] if attn else jnp.zeros(out.shape, f32)
    for i in range(NC):
        for r in range(NX):
            if attn:
                head = mod(p[3] + i, NC) * 2
                pair = [rows[0][(head + h) * NX + mod(p[2] - r, NX)] for h in range(2)]
                part = jnp.concatenate(pair, axis=0).T
            else:
                part = rows[r][:, i * half : (i + 1) * half]
            total = total + jnp.dot(part, weights[i * NX + r][...], preferred_element_type=f32)
    out[...] = total.astype(out.dtype)


def local(
    activations,
    in_gain,
    w_pool_in,
    pool_gain,
    w_qlat,
    w_kvlat,
    w_krope,
    qlat_gain,
    kvlat_gain,
    w_qup,
    w_kup,
    w_vup,
    qhead_gain,
    khead_gain,
    w_out_pool,
    w_out_attn,
):
    at_z, at_y, at_x, at_c = (lax.axis_index(a) for a in ("z", "y", "x", "c"))
    place = jnp.stack([at_z, at_y, at_x, at_c]).astype(jnp.int32)

    normed = row_norm(activations, in_gain).astype(bf16)
    arrived = [normed] + [shift(normed, "x", k) for k in range(1, NX)]
    (normed, w_kvlat, w_qlat, w_kup, w_vup, w_qup) = lax.optimization_barrier(
        (normed, w_kvlat, w_qlat, w_kup, w_vup, w_qup)
    )
    token = jnp.arange(OWN, dtype=jnp.int32)
    positions = (at_z * NY + at_y) * WIDE + (token // ROWS) * (NC * ROWS) + at_c * ROWS + token % ROWS

    def beside(w):
        return w, shift(w, "c", 1)

    down, kv_up, q_up = on_chip(
        arrange_kernel,
        (
            struct(KEY_WIDTH + ROPE + QUERY_WIDTH, activations.shape[1]),
            struct(NY * (NOPE + VDIM), KVLAT),
            struct(NY * HEAD, QLAT),
        ),
        place, *beside(w_kvlat), *beside(w_qlat), w_krope, *beside(w_kup), *beside(w_vup), *beside(w_qup),
    )
    frequency = rope_theta ** (-jnp.arange(0, ROPE, 2, dtype=f32) / ROPE)
    angles = frequency[:, None] * positions.astype(f32)[None, :]
    cosine, sine = jnp.cos(angles), jnp.sin(angles)
    kv_gain, q_gain, k_gain, qh_gain = (g[None] for g in (kvlat_gain, qlat_gain, khead_gain, qhead_gain))
    down, cosine, sine, kv_gain, q_gain, k_gain, qh_gain = lax.optimization_barrier(
        (down, cosine, sine, kv_gain, q_gain, k_gain, qh_gain)
    )

    rows, kv_part, rope_key, q_part = on_chip(
        project_kernel,
        (
            struct(OWN, activations.shape[1]),
            struct(KEY_WIDTH, OWN),
            struct(ROPE, OWN),
            struct(QUERY_WIDTH, OWN),
        ),
        place, *arrived, down,
    )

    kv_parts = [kv_part] + [shift(kv_part, "x", k) for k in range(1, NX)]
    key_values = on_chip(
        key_kernel,
        (struct(HEAD + VDIM, OWN),) * NY,
        place, *kv_parts, rope_key, kv_up, kv_gain, k_gain, cosine, sine,
        scratch=(pltpu.VMEM((KVLAT, OWN), f32), pltpu.VMEM((NY * (NOPE + VDIM), OWN), f32)),
    )
    slots = [key_values[0]] + [shift(key_values[k], "y", k) for k in range(1, NY)]
    piece = jnp.stack([jnp.concatenate(slots[:2], axis=1), jnp.concatenate(slots[2:], axis=1)])
    piece, rows = lax.optimization_barrier((piece, rows))

    q_parts = [q_part] + [shift(q_part, "x", k) for k in range(1, NX)]
    queries = on_chip(
        query_kernel,
        (struct(HEAD, OWN),) * NY,
        place, *q_parts, q_up, q_gain, qh_gain, cosine, sine,
        scratch=(pltpu.VMEM((QLAT, OWN), f32), pltpu.VMEM((NY * HEAD, OWN), f32)),
    )
    own_w = jnp.concatenate([w_out_pool, w_out_attn], axis=0)
    weights = [own_w] + [shift(own_w, "x", k) for k in range(1, NX)]
    mine = jnp.concatenate([queries[0]] + [shift(queries[k], "y", k) for k in range(1, NY)], axis=1)
    other = shift(mine, "c", 1)

    pool_cols = jnp.concatenate(beside(w_pool_in), axis=1)
    pool_in = jnp.dot(rows, pool_cols, preferred_element_type=f32).astype(bf16)
    pool_w = pool_in.shape[1]
    strips = pool_in.reshape(NX, ROWS, pool_w)
    tails = strips[:, ROWS - RIM :]
    across = shift(tails, "c", 1)
    route = [((g - 1) * NC + 1, g * NC) for g in range(1, NZ * NY)]
    far = lax.ppermute(tails[NX - 1], ("z", "y", "c"), route)
    across = jnp.concatenate([across[..., pool_w // 2 :], across[..., : pool_w // 2]], axis=-1)
    far = jnp.concatenate([far[..., pool_w // 2 :], far[..., : pool_w // 2]], axis=-1)
    before = jnp.where(at_c == 1, across, jnp.concatenate([far[None], across[: NX - 1]], axis=0))
    sums = jnp.concatenate([before, strips], axis=1).astype(f32)
    pooled_sums = []
    for reach in (1, 2, 4, 8):
        sums = sums[:, reach:] + sums[:, :-reach]
        pooled_sums.append(sums[:, sums.shape[1] - ROWS :])
    chosen = pooled_sums[-1]
    for level in range(3):
        chosen = jnp.where(at_x == level, pooled_sums[level], chosen)
    divisor = jnp.minimum(positions + 1, jnp.left_shift(2, at_x)).astype(f32).reshape(NX, ROWS, 1)
    pooled = chosen / divisor - strips.astype(f32)
    pool_out = (pooled * jnp.concatenate(beside(pool_gain))).astype(bf16)
    pool_rows = [pick(pool_out, at_x)] + [shift(pick(pool_out, (at_x + k) % NX), "x", k) for k in range(1, NX)]
    up, down, state = piece, piece, None
    for step in range(1, NZ // 2):
        up, down = shift(up, "z", 1), shift(down, "z", -1)
        own = [piece] if step == 1 else []
        state = attend(mine, other, own + [up, down], (0,) * len(own) + (-step, step), place, state)
    state, *weights = lax.optimization_barrier((state, *weights))
    weights += [shift(w, "c", 1) for w in weights]
    end = shift(up, "z", 1)
    here, there = attend(mine, other, [end], (NZ // 2,), place, state, last=True)
    there = shift(there, "c", 1)
    pool_term = on_chip(
        lambda *refs: output_kernel(False, *refs),
        struct(ROWS, activations.shape[1], dtype=f32),
        place, *pool_rows, *weights,
        specs=[WHOLE] * NX + [HALVES[0]] * (NC * NX),
    )

    attended = on_chip(merge_kernel, struct(NY * NX, VDIM, ROWS), place, here, there)
    attn_rows = lax.all_to_all(attended, ("y", "x"), 0, 0, tiled=True)
    return on_chip(
        lambda *refs: output_kernel(True, *refs),
        struct(ROWS, activations.shape[1]),
        place, attn_rows, *weights, pool_term,
        specs=[WHOLE] + [HALVES[1]] * (NC * NX) + [WHOLE],
    )


def solution(mesh):
    fine = Mesh(mesh.devices.reshape(NZ, NY, NX, NC), ("z", "y", "x", "c"))
    tp = ("x", "c")
    every = ("z", "y", "x", "c")
    placed = (
        P(every, None),
        P(),
        P(None, tp),
        P(tp),
        P(None, tp),
        P(None, tp),
        P(),
        P(),
        P(),
        P(None, tp),
        P(None, tp),
        P(None, tp),
        P(),
        P(),
        P(tp, None),
        P(tp, None),
    )

    return jax.shard_map(local, mesh=fine, in_specs=placed, out_specs=P(every, None), check_vma=False)
```

```python
import math

import jax
import jax.numpy as jnp
from jax import lax
from jax.experimental import pallas as pl
from jax.experimental.pallas import tpu as pltpu
from jax.sharding import Mesh, PartitionSpec as P

NOPE = 64
ROPE = 32
HEAD = NOPE + ROPE
VDIM = 64
QLAT = 768
KVLAT = 512
NZ, NY, NX, NC = 8, 4, 4, 2
ROWS = 96
OWN = NX * ROWS
BLOCK = OWN * NY
QUERIES = NC * BLOCK
WIDE = NC * OWN
CHUNK = 256
VROWS = VDIM + 16
DEPTH = 128
RIM = 16

norm_eps = 1e-06
rope_theta = 10000.0
bf16 = jnp.bfloat16
f32 = jnp.float32


def shift(x, axis, distance):
    n = lax.axis_size(axis)
    return lax.ppermute(x, axis, [(i, (i + distance) % n) for i in range(n)])


def pick(x, i):
    return lax.dynamic_index_in_dim(x, i, 0, keepdims=False)


def row_norm(source, gain):
    as_float = source.astype(f32)
    factor = lax.rsqrt(jnp.mean(as_float * as_float, axis=-1, keepdims=True) + norm_eps)
    return as_float * factor * gain


def turned(lower, upper, cosine, sine):
    return lower * cosine - upper * sine, upper * cosine + lower * sine


def attend_kernel(steps, first, last, p, own_ref, other_ref, *refs):
    pieces, refs = refs[: len(steps)], refs[len(steps) :]
    if not first:
        state_ref, refs = refs[0], refs[1:]
    outs, scratch = refs[: 2 if last else 1], refs[2 if last else 1 :]
    acc_ref, q_ref, k_ref, v_ref, half_ref, raw_ref, piece_sem, query_sem, state_sem, out_sem = scratch
    here_z, here_y, core = p[0], p[1], p[3]
    loads = [pltpu.make_async_copy(piece, raw_ref.at[b], piece_sem.at[b]) for b, piece in enumerate(pieces)]
    queries = [pltpu.make_async_copy(r, half_ref.at[i], query_sem.at[i]) for i, r in enumerate((own_ref, other_ref))]
    for copy in loads[:1] + queries:
        copy.start()
    if not first:
        state_load = pltpu.make_async_copy(state_ref, acc_ref, state_sem)
        state_load.start()
    for copy in loads[1:]:
        copy.start()
    q_ref[HEAD:DEPTH, :] = jnp.zeros((DEPTH - HEAD, QUERIES), bf16)
    k_ref[:, HEAD:DEPTH] = jnp.zeros((BLOCK, DEPTH - HEAD), bf16)
    v_ref[VDIM:VROWS, :] = jnp.ones((VROWS - VDIM, BLOCK), bf16)
    if first:
        acc_ref[...] = jnp.zeros_like(acc_ref)

    def strips(u):
        return u + ROWS * sum((u >= ROWS * n).astype(jnp.int32) for n in range(1, NX))

    def key_places(i):
        at = i * CHUNK + lax.broadcasted_iota(jnp.int32, (CHUNK, 1), 0)
        lo, hi = i * CHUNK // OWN, ((i + 1) * CHUNK - 1) // OWN
        place = strips(at - lo * OWN) + WIDE * lax.rem(here_y - lo + NY, NY)
        if hi > lo:
            place = jnp.where(at < hi * OWN, place, strips(at - hi * OWN) + WIDE * lax.rem(here_y - hi + NY, NY))
        return place + core * ROWS

    def add(off, g_y, lead):
        masked = first
        q = q_ref[:, pl.ds(off, WIDE)]
        out = acc_ref[:, pl.ds(off, WIDE)]
        if masked:
            at = lax.broadcasted_iota(jnp.int32, (1, WIDE), 1)
            q_place = jnp.where(at < OWN, strips(at) + core * ROWS, strips(at - OWN) + (1 - core) * ROWS)
            q_place = q_place + (WIDE * g_y + lead)
        n = BLOCK // CHUNK
        s = jnp.dot(k_ref[0:CHUNK, :], q, preferred_element_type=f32)
        for i in range(n):
            ahead = None
            if i + 1 < n:
                ahead = jnp.dot(k_ref[(i + 1) * CHUNK : (i + 2) * CHUNK, :], q, preferred_element_type=f32)
            weights = jnp.exp2(s)
            if masked:
                weights = jnp.where(key_places(i) <= q_place, weights, 0.0)
            out = out + jnp.dot(v_ref[:, i * CHUNK : (i + 1) * CHUNK], weights.astype(bf16), preferred_element_type=f32)
            s = ahead
        acc_ref[:, pl.ds(off, WIDE)] = out

    for copy in loads:
        copy.wait()
    for copy in queries:
        copy.wait()
    for g in range(NY):
        for half in range(NC):
            q_ref[0:HEAD, g * WIDE + half * OWN : g * WIDE + (half + 1) * OWN] = half_ref[half, :, g * OWN : (g + 1) * OWN]
    if not first:
        state_load.wait()

    def piece_add(b, lead):
        for i in range(2):
            cut = BLOCK // 2
            k_ref[i * cut : (i + 1) * cut, 0:HEAD] = raw_ref[b, i, 0:HEAD, :].T
            v_ref[0:VDIM, i * cut : (i + 1) * cut] = raw_ref[b, i, HEAD : HEAD + VDIM, :]

        def group(g, inner):
            add(pl.multiple_of(g * WIDE, WIDE), mod(here_y - g, NY), lead)
            return inner

        lax.fori_loop(0, NY, group, 0)

    def piece_step(b, carry):
        step = jnp.int32(steps[-1])
        for i in range(len(steps) - 1):
            step = jnp.where(b == i, steps[i], step)
        block_z = mod(here_z + step, NZ)
        pl.when(block_z <= here_z)(lambda: piece_add(b, jnp.where(block_z < here_z, NY * WIDE, 0)))
        return carry

    lax.fori_loop(0, len(steps), piece_step, 0)
    stores = []
    if last:
        for g in range(NY):
            for half, ref in enumerate(outs):
                source = acc_ref.at[0 : VDIM + 8, g * WIDE + half * OWN : g * WIDE + (half + 1) * OWN]
                target = ref.at[:, g * OWN : (g + 1) * OWN]
                stores.append(pltpu.make_async_copy(source, target, out_sem.at[g, half]))
    else:
        for g in range(NY):
            cut = slice(g * WIDE, (g + 1) * WIDE)
            stores.append(pltpu.make_async_copy(acc_ref.at[:, cut], outs[0].at[:, cut], out_sem.at[g, 0]))
    for copy in stores:
        copy.start()
    for copy in stores:
        copy.wait()


def attend(own, other, pieces, steps, place, state, last=False):
    first = state is None
    anywhere = pl.BlockSpec(memory_space=pl.ANY)
    operands = [place, own, other, *pieces] + ([] if first else [state])
    half = jax.ShapeDtypeStruct((VDIM + 8, BLOCK), f32)
    count = len(steps)
    return pl.pallas_call(
        lambda *refs: attend_kernel(steps, first, last, *refs),
        out_shape=(half, half) if last else jax.ShapeDtypeStruct((VROWS, QUERIES), f32),
        in_specs=[pl.BlockSpec(memory_space=pltpu.SMEM)] + [anywhere] * (len(operands) - 1),
        out_specs=(anywhere, anywhere) if last else anywhere,
        scratch_shapes=[
            pltpu.VMEM((VROWS, QUERIES), f32),
            pltpu.VMEM((DEPTH, QUERIES), bf16),
            pltpu.VMEM((BLOCK, DEPTH), bf16),
            pltpu.VMEM((VROWS, BLOCK), bf16),
            pltpu.VMEM((NC, HEAD, BLOCK), bf16),
            pltpu.VMEM((count, 2, HEAD + VDIM, BLOCK // 2), bf16),
            pltpu.SemaphoreType.DMA((count,)),
            pltpu.SemaphoreType.DMA((NC,)),
            pltpu.SemaphoreType.DMA,
            pltpu.SemaphoreType.DMA((NY, NC)),
        ],
        cost_estimate=pl.CostEstimate(
            flops=4 * count * QUERIES * BLOCK * 256, transcendentals=count * QUERIES * BLOCK, bytes_accessed=4 << 20
        ),
        name="attend",
    )(*operands)


WHOLE = pl.BlockSpec(memory_space=pltpu.VMEM)
SCALARS = pl.BlockSpec(memory_space=pltpu.SMEM)
HALVES = [pl.BlockSpec((128, 2048), lambda i, h=h: (h, 0)) for h in range(2)]
KEY_WIDTH = NC * KVLAT // (NX * NC)
QUERY_WIDTH = NC * QLAT // (NX * NC)


def on_chip(kernel, outs, place, *operands, scratch=(), flops=1 << 30, specs=None):
    return pl.pallas_call(
        kernel,
        out_shape=outs,
        grid=(1,) if specs else (),
        in_specs=[SCALARS] + (specs or [WHOLE] * len(operands)),
        out_specs=jax.tree.map(lambda _: WHOLE, outs),
        scratch_shapes=list(scratch),
        cost_estimate=pl.CostEstimate(flops=flops, transcendentals=0, bytes_accessed=4 << 20),
    )(place, *operands)


def struct(*shape, dtype=bf16):
    return jax.ShapeDtypeStruct(shape, dtype)


def mod(i, n):
    return lax.rem(i + n, n)


def arrange_kernel(p, kv, kv_o, q, q_o, rope, kup, kup_o, vup, vup_o, qup, qup_o, down_ref, kv_ref, q_ref):
    core = p[3]
    width, wide = KEY_WIDTH // NC, QUERY_WIDTH // NC

    def some(n, carry):
        cut = pl.ds(pl.multiple_of(n * 512, 512), 512)
        for i, (mine, there) in enumerate(((kv, q), (kv_o, q_o))):
            c = mod(core + i, NC)
            down_ref[pl.ds(pl.multiple_of(c * width, width), width), cut] = mine[cut, :].T
            down_ref[pl.ds(pl.multiple_of(KEY_WIDTH + ROPE + c * wide, ROPE), wide), cut] = there[cut, :].T
        down_ref[KEY_WIDTH : KEY_WIDTH + ROPE, cut] = rope[cut, :].T
        return carry

    lax.fori_loop(0, rope.shape[0] // 512, some, 0)
    for i, (k, v, w) in enumerate(((kup, vup, qup), (kup_o, vup_o, qup_o))):
        c = mod(core + i, NC)
        k, v, w = k[...].T, v[...].T, w[...].T
        for h in range(2):
            m = c * 2 + h
            both = NOPE + VDIM
            kv_ref[pl.ds(pl.multiple_of(m * both, both), NOPE), :] = k[h * NOPE : (h + 1) * NOPE]
            kv_ref[pl.ds(pl.multiple_of(m * both + NOPE, NOPE), VDIM), :] = v[h * VDIM : (h + 1) * VDIM]
            q_ref[pl.ds(pl.multiple_of(m * HEAD, ROPE), HEAD), :] = w[h * HEAD : (h + 1) * HEAD]


def project_kernel(p, b0, b1, b2, b3, w, rows_ref, kv_ref, rope_ref, q_ref):
    x = p[2]
    for k, block in enumerate((b0, b1, b2, b3)):
        at = pl.multiple_of(mod(x - k, NX) * ROWS, ROPE)
        rows_ref[pl.ds(at, ROWS), :] = block[...]
    out = lax.dot_general(w[...], rows_ref[...], (((1,), (1,)), ((), ())), preferred_element_type=f32).astype(bf16)
    kv_ref[...] = out[:KEY_WIDTH]
    rope_ref[...] = out[KEY_WIDTH : KEY_WIDTH + ROPE]
    q_ref[...] = out[KEY_WIDTH + ROPE :]


def column(row_ref):
    return jnp.broadcast_to(row_ref[...], (8, row_ref.shape[1])).T[:, 0:1]


def latent_rows(p, parts, lat_ref, gain):
    x = p[2]
    width = parts[0].shape[0]
    for r, part in enumerate(parts):
        lat_ref[pl.ds(pl.multiple_of(mod(x - r, NX) * width, 64), width), :] = part[...].astype(f32)
    lat = lat_ref[...]
    factor = lax.rsqrt(jnp.mean(lat * lat, axis=0, keepdims=True) + norm_eps)
    return (lat * factor * column(gain)).astype(bf16)


def key_kernel(p, p0, p1, p2, p3, rope_ref, w, gain, head_gain, cos, sin, o0, o1, o2, o3, lat_ref, up_ref):
    normed = latent_rows(p, (p0, p1, p2, p3), lat_ref, gain)
    up_ref[...] = jnp.dot(w[...], normed, preferred_element_type=f32).astype(bf16).astype(f32)
    head_gain = column(head_gain)
    rope = rope_ref[...].astype(f32)
    rope_squares = jnp.sum(rope * rope, axis=0, keepdims=True)
    both = NOPE + VDIM
    for k, out in enumerate((o0, o1, o2, o3)):
        m = mod(p[1] + k, NY)
        plain = up_ref[pl.ds(pl.multiple_of(m * both, both), NOPE), :]
        factor = lax.rsqrt((jnp.sum(plain * plain, axis=0, keepdims=True) + rope_squares) / HEAD + norm_eps)
        out[0:NOPE, :] = (plain * factor * head_gain[0:NOPE]).astype(bf16)
        part = rope * factor * head_gain[NOPE:HEAD]
        low, high = turned(part[: ROPE // 2], part[ROPE // 2 :], cos[...], sin[...])
        out[NOPE : NOPE + ROPE // 2, :] = low.astype(bf16)
        out[NOPE + ROPE // 2 : HEAD, :] = high.astype(bf16)
        out[HEAD:, :] = up_ref[pl.ds(pl.multiple_of(m * both + NOPE, NOPE), VDIM), :].astype(bf16)


def query_kernel(p, p0, p1, p2, p3, w, gain, head_gain, cos, sin, o0, o1, o2, o3, lat_ref, up_ref):
    normed = latent_rows(p, (p0, p1, p2, p3), lat_ref, gain)
    up_ref[...] = jnp.dot(w[...], normed, preferred_element_type=f32).astype(bf16).astype(f32)
    scale = column(head_gain) * (HEAD**-0.5 * math.log2(math.e))
    for k, out in enumerate((o0, o1, o2, o3)):
        m = mod(p[1] + k, NY)
        raw = up_ref[pl.ds(pl.multiple_of(m * HEAD, ROPE), HEAD), :]
        factor = lax.rsqrt(jnp.mean(raw * raw, axis=0, keepdims=True) + norm_eps)
        part = raw * factor * scale
        low, high = turned(part[NOPE : NOPE + ROPE // 2], part[NOPE + ROPE // 2 :], cos[...], sin[...])
        out[0:NOPE, :] = part[:NOPE].astype(bf16)
        out[NOPE : NOPE + ROPE // 2, :] = low.astype(bf16)
        out[NOPE + ROPE // 2 :, :] = high.astype(bf16)


def merge_kernel(p, here, there, out):
    total = here[...] + there[...]
    result = (total[:VDIM] / total[VDIM : VDIM + 1]).astype(bf16)
    for k in range(NY):
        y = mod(p[1] - k, NY)
        for x in range(NX):
            out[y * NX + x] = result[:, k * OWN + x * ROWS : k * OWN + (x + 1) * ROWS]


def output_kernel(attn, p, *refs):
    rows, refs = (refs[:1], refs[1:]) if attn else (refs[:NX], refs[NX:])
    weights, refs = refs[: NC * NX], refs[NC * NX :]
    out = refs[-1]
    half = weights[0].shape[0]
    total = refs[0][...] if attn else jnp.zeros(out.shape, f32)
    for i in range(NC):
        for r in range(NX):
            if attn:
                head = mod(p[3] + i, NC) * 2
                pair = [rows[0][(head + h) * NX + mod(p[2] - r, NX)] for h in range(2)]
                part = jnp.concatenate(pair, axis=0).T
            else:
                part = rows[r][:, i * half : (i + 1) * half]
            total = total + jnp.dot(part, weights[i * NX + r][...], preferred_element_type=f32)
    out[...] = total.astype(out.dtype)


def local(
    activations,
    in_gain,
    w_pool_in,
    pool_gain,
    w_qlat,
    w_kvlat,
    w_krope,
    qlat_gain,
    kvlat_gain,
    w_qup,
    w_kup,
    w_vup,
    qhead_gain,
    khead_gain,
    w_out_pool,
    w_out_attn,
):
    at_z, at_y, at_x, at_c = (lax.axis_index(a) for a in ("z", "y", "x", "c"))
    place = jnp.stack([at_z, at_y, at_x, at_c]).astype(jnp.int32)

    normed = row_norm(activations, in_gain).astype(bf16)
    arrived = [normed] + [shift(normed, "x", k) for k in range(1, NX)]
    (normed, w_kvlat, w_qlat, w_kup, w_vup, w_qup) = lax.optimization_barrier(
        (normed, w_kvlat, w_qlat, w_kup, w_vup, w_qup)
    )
    token = jnp.arange(OWN, dtype=jnp.int32)
    positions = (at_z * NY + at_y) * WIDE + (token // ROWS) * (NC * ROWS) + at_c * ROWS + token % ROWS

    def beside(w):
        return w, shift(w, "c", 1)

    down, kv_up, q_up = on_chip(
        arrange_kernel,
        (
            struct(KEY_WIDTH + ROPE + QUERY_WIDTH, activations.shape[1]),
            struct(NY * (NOPE + VDIM), KVLAT),
            struct(NY * HEAD, QLAT),
        ),
        place, *beside(w_kvlat), *beside(w_qlat), w_krope, *beside(w_kup), *beside(w_vup), *beside(w_qup),
    )
    frequency = rope_theta ** (-jnp.arange(0, ROPE, 2, dtype=f32) / ROPE)
    angles = frequency[:, None] * positions.astype(f32)[None, :]
    cosine, sine = jnp.cos(angles), jnp.sin(angles)
    kv_gain, q_gain, k_gain, qh_gain = (g[None] for g in (kvlat_gain, qlat_gain, khead_gain, qhead_gain))
    down, cosine, sine, kv_gain, q_gain, k_gain, qh_gain = lax.optimization_barrier(
        (down, cosine, sine, kv_gain, q_gain, k_gain, qh_gain)
    )

    rows, kv_part, rope_key, q_part = on_chip(
        project_kernel,
        (
            struct(OWN, activations.shape[1]),
            struct(KEY_WIDTH, OWN),
            struct(ROPE, OWN),
            struct(QUERY_WIDTH, OWN),
        ),
        place, *arrived, down,
    )

    kv_parts = [kv_part] + [shift(kv_part, "x", k) for k in range(1, NX)]
    key_values = on_chip(
        key_kernel,
        (struct(HEAD + VDIM, OWN),) * NY,
        place, *kv_parts, rope_key, kv_up, kv_gain, k_gain, cosine, sine,
        scratch=(pltpu.VMEM((KVLAT, OWN), f32), pltpu.VMEM((NY * (NOPE + VDIM), OWN), f32)),
    )
    slots = [key_values[0]] + [shift(key_values[k], "y", k) for k in range(1, NY)]
    piece = jnp.stack([jnp.concatenate(slots[:2], axis=1), jnp.concatenate(slots[2:], axis=1)])
    piece, rows = lax.optimization_barrier((piece, rows))

    q_parts = [q_part] + [shift(q_part, "x", k) for k in range(1, NX)]
    queries = on_chip(
        query_kernel,
        (struct(HEAD, OWN),) * NY,
        place, *q_parts, q_up, q_gain, qh_gain, cosine, sine,
        scratch=(pltpu.VMEM((QLAT, OWN), f32), pltpu.VMEM((NY * HEAD, OWN), f32)),
    )
    own_w = jnp.concatenate([w_out_pool, w_out_attn], axis=0)
    weights = [own_w] + [shift(own_w, "x", k) for k in range(1, NX)]
    mine = jnp.concatenate([queries[0]] + [shift(queries[k], "y", k) for k in range(1, NY)], axis=1)
    other = shift(mine, "c", 1)

    pool_cols = jnp.concatenate(beside(w_pool_in), axis=1)
    pool_in = jnp.dot(rows, pool_cols, preferred_element_type=f32).astype(bf16)
    pool_w = pool_in.shape[1]
    strips = pool_in.reshape(NX, ROWS, pool_w)
    tails = strips[:, ROWS - RIM :]
    across = shift(tails, "c", 1)
    route = [((g - 1) * NC + 1, g * NC) for g in range(1, NZ * NY)]
    far = lax.ppermute(tails[NX - 1], ("z", "y", "c"), route)
    across = jnp.concatenate([across[..., pool_w // 2 :], across[..., : pool_w // 2]], axis=-1)
    far = jnp.concatenate([far[..., pool_w // 2 :], far[..., : pool_w // 2]], axis=-1)
    before = jnp.where(at_c == 1, across, jnp.concatenate([far[None], across[: NX - 1]], axis=0))
    sums = jnp.concatenate([before, strips], axis=1).astype(f32)
    pooled_sums = []
    for reach in (1, 2, 4, 8):
        sums = sums[:, reach:] + sums[:, :-reach]
        pooled_sums.append(sums[:, sums.shape[1] - ROWS :])
    chosen = pooled_sums[-1]
    for level in range(3):
        chosen = jnp.where(at_x == level, pooled_sums[level], chosen)
    divisor = jnp.minimum(positions + 1, jnp.left_shift(2, at_x)).astype(f32).reshape(NX, ROWS, 1)
    pooled = chosen / divisor - strips.astype(f32)
    pool_out = (pooled * jnp.concatenate(beside(pool_gain))).astype(bf16)
    pool_rows = [pick(pool_out, at_x)] + [shift(pick(pool_out, (at_x + k) % NX), "x", k) for k in range(1, NX)]
    up, down, state = piece, piece, None
    for step in range(1, NZ // 2):
        up, down = shift(up, "z", 1), shift(down, "z", -1)
        own = [piece] if step == 1 else []
        state = attend(mine, other, own + [up, down], (0,) * len(own) + (-step, step), place, state)
    state, *weights = lax.optimization_barrier((state, *weights))
    weights += [shift(w, "c", 1) for w in weights]
    end = shift(up, "z", 1)
    here, there = attend(mine, other, [end], (NZ // 2,), place, state, last=True)
    there = shift(there, "c", 1)
    pool_term = on_chip(
        lambda *refs: output_kernel(False, *refs),
        struct(ROWS, activations.shape[1], dtype=f32),
        place, *pool_rows, *weights,
        specs=[WHOLE] * NX + [HALVES[0]] * (NC * NX),
    )

    attended = on_chip(merge_kernel, struct(NY * NX, VDIM, ROWS), place, here, there)
    attn_rows = lax.all_to_all(attended, ("y", "x"), 0, 0, tiled=True)
    return on_chip(
        lambda *refs: output_kernel(True, *refs),
        struct(ROWS, activations.shape[1]),
        place, attn_rows, *weights, pool_term,
        specs=[WHOLE] + [HALVES[1]] * (NC * NX) + [WHOLE],
    )


def solution(mesh):
    fine = Mesh(mesh.devices.reshape(NZ, NY, NX, NC), ("z", "y", "x", "c"))
    tp = ("x", "c")
    every = ("z", "y", "x", "c")
    placed = (
        P(every, None),
        P(),
        P(None, tp),
        P(tp),
        P(None, tp),
        P(None, tp),
        P(),
        P(),
        P(),
        P(None, tp),
        P(None, tp),
        P(None, tp),
        P(),
        P(),
        P(tp, None),
        P(tp, None),
    )

    return jax.shard_map(local, mesh=fine, in_specs=placed, out_specs=P(every, None), check_vma=False)
```

```python
import math

import jax
import jax.numpy as jnp
from jax import lax
from jax.experimental import pallas as pl
from jax.experimental.pallas import tpu as pltpu
from jax.sharding import Mesh, PartitionSpec as P

NOPE = 64
ROPE = 32
HEAD = NOPE + ROPE
VDIM = 64
QLAT = 768
KVLAT = 512
NZ, NY, NX, NC = 8, 4, 4, 2
ROWS = 96
OWN = NX * ROWS
BLOCK = OWN * NY
QUERIES = NC * BLOCK
WIDE = NC * OWN
CHUNK = 256
VROWS = VDIM + 16
DEPTH = 128
RIM = 16

norm_eps = 1e-06
rope_theta = 10000.0
bf16 = jnp.bfloat16
f32 = jnp.float32


def shift(x, axis, distance):
    n = lax.axis_size(axis)
    return lax.ppermute(x, axis, [(i, (i + distance) % n) for i in range(n)])


def pick(x, i):
    return lax.dynamic_index_in_dim(x, i, 0, keepdims=False)


def row_norm(source, gain):
    as_float = source.astype(f32)
    factor = lax.rsqrt(jnp.mean(as_float * as_float, axis=-1, keepdims=True) + norm_eps)
    return as_float * factor * gain


def turned(lower, upper, cosine, sine):
    return lower * cosine - upper * sine, upper * cosine + lower * sine


def attend_kernel(steps, first, last, p, own_ref, other_ref, *refs):
    pieces, refs = refs[: len(steps)], refs[len(steps) :]
    if not first:
        state_ref, refs = refs[0], refs[1:]
    outs, scratch = refs[: 2 if last else 1], refs[2 if last else 1 :]
    acc_ref, q_ref, k_ref, v_ref, half_ref, raw_ref, piece_sem, query_sem, state_sem, out_sem = scratch
    here_z, here_y, core = p[0], p[1], p[3]
    loads = [pltpu.make_async_copy(piece, raw_ref.at[b], piece_sem.at[b]) for b, piece in enumerate(pieces)]
    queries = [pltpu.make_async_copy(r, half_ref.at[i], query_sem.at[i]) for i, r in enumerate((own_ref, other_ref))]
    for copy in loads[:1] + queries:
        copy.start()
    if not first:
        state_load = pltpu.make_async_copy(state_ref, acc_ref, state_sem)
        state_load.start()
    for copy in loads[1:]:
        copy.start()
    q_ref[HEAD:DEPTH, :] = jnp.zeros((DEPTH - HEAD, QUERIES), bf16)
    k_ref[:, HEAD:DEPTH] = jnp.zeros((BLOCK, DEPTH - HEAD), bf16)
    v_ref[VDIM:VROWS, :] = jnp.ones((VROWS - VDIM, BLOCK), bf16)
    if first:
        acc_ref[...] = jnp.zeros_like(acc_ref)

    def strips(u):
        return u + ROWS * sum((u >= ROWS * n).astype(jnp.int32) for n in range(1, NX))

    def key_places(i):
        at = i * CHUNK + lax.broadcasted_iota(jnp.int32, (CHUNK, 1), 0)
        lo, hi = i * CHUNK // OWN, ((i + 1) * CHUNK - 1) // OWN
        place = strips(at - lo * OWN) + WIDE * lax.rem(here_y - lo + NY, NY)
        if hi > lo:
            place = jnp.where(at < hi * OWN, place, strips(at - hi * OWN) + WIDE * lax.rem(here_y - hi + NY, NY))
        return place + core * ROWS

    def add(off, g_y, lead):
        masked = first
        q = q_ref[:, pl.ds(off, WIDE)]
        out = acc_ref[:, pl.ds(off, WIDE)]
        if masked:
            at = lax.broadcasted_iota(jnp.int32, (1, WIDE), 1)
            q_place = jnp.where(at < OWN, strips(at) + core * ROWS, strips(at - OWN) + (1 - core) * ROWS)
            q_place = q_place + (WIDE * g_y + lead)
        n = BLOCK // CHUNK
        s = jnp.dot(k_ref[0:CHUNK, :], q, preferred_element_type=f32)
        for i in range(n):
            ahead = None
            if i + 1 < n:
                ahead = jnp.dot(k_ref[(i + 1) * CHUNK : (i + 2) * CHUNK, :], q, preferred_element_type=f32)
            weights = jnp.exp2(s)
            if masked:
                weights = jnp.where(key_places(i) <= q_place, weights, 0.0)
            out = out + jnp.dot(v_ref[:, i * CHUNK : (i + 1) * CHUNK], weights.astype(bf16), preferred_element_type=f32)
            s = ahead
        acc_ref[:, pl.ds(off, WIDE)] = out

    for copy in queries:
        copy.wait()
    for g in range(NY):
        for half in range(NC):
            q_ref[0:HEAD, g * WIDE + half * OWN : g * WIDE + (half + 1) * OWN] = half_ref[half, :, g * OWN : (g + 1) * OWN]
    if not first:
        state_load.wait()

    def store(g):
        off, small = pl.multiple_of(g * WIDE, WIDE), pl.multiple_of(g * OWN, OWN)
        if not last:
            cut = pl.ds(off, WIDE)
            return [pltpu.make_async_copy(acc_ref.at[:, cut], outs[0].at[:, cut], out_sem.at[g, 0])]
        return [
            pltpu.make_async_copy(
                acc_ref.at[0 : VDIM + 8, pl.ds(pl.multiple_of(off + half * OWN, OWN), OWN)],
                ref.at[:, pl.ds(small, OWN)],
                out_sem.at[g, half],
            )
            for half, ref in enumerate(outs)
        ]

    def piece_step(b, carry):
        step = jnp.int32(steps[-1])
        for i in range(len(steps) - 1):
            step = jnp.where(b == i, steps[i], step)
        for i, copy in enumerate(loads):
            pl.when(b == i)(copy.wait)
        block_z = mod(here_z + step, NZ)
        needed = block_z <= here_z
        lead = jnp.where(block_z < here_z, NY * WIDE, 0)

        @pl.when(needed)
        def _():
            for i in range(2):
                cut = BLOCK // 2
                k_ref[i * cut : (i + 1) * cut, 0:HEAD] = raw_ref[b, i, 0:HEAD, :].T
                v_ref[0:VDIM, i * cut : (i + 1) * cut] = raw_ref[b, i, HEAD : HEAD + VDIM, :]

        def group(g, inner):
            pl.when(needed)(lambda: add(pl.multiple_of(g * WIDE, WIDE), mod(here_y - g, NY), lead))

            @pl.when(b == len(steps) - 1)
            def _():
                for copy in store(g):
                    copy.start()

            return inner

        lax.fori_loop(0, NY, group, 0)
        return carry

    lax.fori_loop(0, len(steps), piece_step, 0)
    for g in range(NY):
        for copy in store(g):
            copy.wait()


def attend(own, other, pieces, steps, place, state, last=False):
    first = state is None
    anywhere = pl.BlockSpec(memory_space=pl.ANY)
    operands = [place, own, other, *pieces] + ([] if first else [state])
    half = jax.ShapeDtypeStruct((VDIM + 8, BLOCK), f32)
    count = len(steps)
    return pl.pallas_call(
        lambda *refs: attend_kernel(steps, first, last, *refs),
        out_shape=(half, half) if last else jax.ShapeDtypeStruct((VROWS, QUERIES), f32),
        in_specs=[pl.BlockSpec(memory_space=pltpu.SMEM)] + [anywhere] * (len(operands) - 1),
        out_specs=(anywhere, anywhere) if last else anywhere,
        scratch_shapes=[
            pltpu.VMEM((VROWS, QUERIES), f32),
            pltpu.VMEM((DEPTH, QUERIES), bf16),
            pltpu.VMEM((BLOCK, DEPTH), bf16),
            pltpu.VMEM((VROWS, BLOCK), bf16),
            pltpu.VMEM((NC, HEAD, BLOCK), bf16),
            pltpu.VMEM((count, 2, HEAD + VDIM, BLOCK // 2), bf16),
            pltpu.SemaphoreType.DMA((count,)),
            pltpu.SemaphoreType.DMA((NC,)),
            pltpu.SemaphoreType.DMA,
            pltpu.SemaphoreType.DMA((NY, NC)),
        ],
        cost_estimate=pl.CostEstimate(
            flops=4 * count * QUERIES * BLOCK * 256, transcendentals=count * QUERIES * BLOCK, bytes_accessed=4 << 20
        ),
        name="attend",
    )(*operands)


WHOLE = pl.BlockSpec(memory_space=pltpu.VMEM)
SCALARS = pl.BlockSpec(memory_space=pltpu.SMEM)
HALVES = [pl.BlockSpec((128, 2048), lambda i, h=h: (h, 0)) for h in range(2)]
KEY_WIDTH = NC * KVLAT // (NX * NC)
QUERY_WIDTH = NC * QLAT // (NX * NC)


def on_chip(kernel, outs, place, *operands, scratch=(), flops=1 << 30, specs=None):
    return pl.pallas_call(
        kernel,
        out_shape=outs,
        grid=(1,) if specs else (),
        in_specs=[SCALARS] + (specs or [WHOLE] * len(operands)),
        out_specs=jax.tree.map(lambda _: WHOLE, outs),
        scratch_shapes=list(scratch),
        cost_estimate=pl.CostEstimate(flops=flops, transcendentals=0, bytes_accessed=4 << 20),
    )(place, *operands)


def struct(*shape, dtype=bf16):
    return jax.ShapeDtypeStruct(shape, dtype)


def mod(i, n):
    return lax.rem(i + n, n)


def arrange_kernel(p, kv, kv_o, q, q_o, rope, kup, kup_o, vup, vup_o, qup, qup_o, down_ref, kv_ref, q_ref):
    core = p[3]
    width, wide = KEY_WIDTH // NC, QUERY_WIDTH // NC

    def some(n, carry):
        cut = pl.ds(pl.multiple_of(n * 512, 512), 512)
        for i, (mine, there) in enumerate(((kv, q), (kv_o, q_o))):
            c = mod(core + i, NC)
            down_ref[pl.ds(pl.multiple_of(c * width, width), width), cut] = mine[cut, :].T
            down_ref[pl.ds(pl.multiple_of(KEY_WIDTH + ROPE + c * wide, ROPE), wide), cut] = there[cut, :].T
        down_ref[KEY_WIDTH : KEY_WIDTH + ROPE, cut] = rope[cut, :].T
        return carry

    lax.fori_loop(0, rope.shape[0] // 512, some, 0)
    for i, (k, v, w) in enumerate(((kup, vup, qup), (kup_o, vup_o, qup_o))):
        c = mod(core + i, NC)
        k, v, w = k[...].T, v[...].T, w[...].T
        for h in range(2):
            m = c * 2 + h
            both = NOPE + VDIM
            kv_ref[pl.ds(pl.multiple_of(m * both, both), NOPE), :] = k[h * NOPE : (h + 1) * NOPE]
            kv_ref[pl.ds(pl.multiple_of(m * both + NOPE, NOPE), VDIM), :] = v[h * VDIM : (h + 1) * VDIM]
            q_ref[pl.ds(pl.multiple_of(m * HEAD, ROPE), HEAD), :] = w[h * HEAD : (h + 1) * HEAD]


def project_kernel(p, b0, b1, b2, b3, w, rows_ref, kv_ref, rope_ref, q_ref):
    x = p[2]
    for k, block in enumerate((b0, b1, b2, b3)):
        at = pl.multiple_of(mod(x - k, NX) * ROWS, ROPE)
        rows_ref[pl.ds(at, ROWS), :] = block[...]
    out = lax.dot_general(w[...], rows_ref[...], (((1,), (1,)), ((), ())), preferred_element_type=f32).astype(bf16)
    kv_ref[...] = out[:KEY_WIDTH]
    rope_ref[...] = out[KEY_WIDTH : KEY_WIDTH + ROPE]
    q_ref[...] = out[KEY_WIDTH + ROPE :]


def column(row_ref):
    return jnp.broadcast_to(row_ref[...], (8, row_ref.shape[1])).T[:, 0:1]


def latent_rows(p, parts, lat_ref, gain):
    x = p[2]
    width = parts[0].shape[0]
    for r, part in enumerate(parts):
        lat_ref[pl.ds(pl.multiple_of(mod(x - r, NX) * width, 64), width), :] = part[...].astype(f32)
    lat = lat_ref[...]
    factor = lax.rsqrt(jnp.mean(lat * lat, axis=0, keepdims=True) + norm_eps)
    return (lat * factor * column(gain)).astype(bf16)


def key_kernel(p, p0, p1, p2, p3, rope_ref, w, gain, head_gain, cos, sin, o0, o1, o2, o3, lat_ref, up_ref):
    normed = latent_rows(p, (p0, p1, p2, p3), lat_ref, gain)
    up_ref[...] = jnp.dot(w[...], normed, preferred_element_type=f32).astype(bf16).astype(f32)
    head_gain = column(head_gain)
    rope = rope_ref[...].astype(f32)
    rope_squares = jnp.sum(rope * rope, axis=0, keepdims=True)
    both = NOPE + VDIM
    for k, out in enumerate((o0, o1, o2, o3)):
        m = mod(p[1] + k, NY)
        plain = up_ref[pl.ds(pl.multiple_of(m * both, both), NOPE), :]
        factor = lax.rsqrt((jnp.sum(plain * plain, axis=0, keepdims=True) + rope_squares) / HEAD + norm_eps)
        out[0:NOPE, :] = (plain * factor * head_gain[0:NOPE]).astype(bf16)
        part = rope * factor * head_gain[NOPE:HEAD]
        low, high = turned(part[: ROPE // 2], part[ROPE // 2 :], cos[...], sin[...])
        out[NOPE : NOPE + ROPE // 2, :] = low.astype(bf16)
        out[NOPE + ROPE // 2 : HEAD, :] = high.astype(bf16)
        out[HEAD:, :] = up_ref[pl.ds(pl.multiple_of(m * both + NOPE, NOPE), VDIM), :].astype(bf16)


def query_kernel(p, p0, p1, p2, p3, w, gain, head_gain, cos, sin, o0, o1, o2, o3, lat_ref, up_ref):
    normed = latent_rows(p, (p0, p1, p2, p3), lat_ref, gain)
    up_ref[...] = jnp.dot(w[...], normed, preferred_element_type=f32).astype(bf16).astype(f32)
    scale = column(head_gain) * (HEAD**-0.5 * math.log2(math.e))
    for k, out in enumerate((o0, o1, o2, o3)):
        m = mod(p[1] + k, NY)
        raw = up_ref[pl.ds(pl.multiple_of(m * HEAD, ROPE), HEAD), :]
        factor = lax.rsqrt(jnp.mean(raw * raw, axis=0, keepdims=True) + norm_eps)
        part = raw * factor * scale
        low, high = turned(part[NOPE : NOPE + ROPE // 2], part[NOPE + ROPE // 2 :], cos[...], sin[...])
        out[0:NOPE, :] = part[:NOPE].astype(bf16)
        out[NOPE : NOPE + ROPE // 2, :] = low.astype(bf16)
        out[NOPE + ROPE // 2 :, :] = high.astype(bf16)


def merge_kernel(p, here, there, out):
    total = here[...] + there[...]
    result = (total[:VDIM] / total[VDIM : VDIM + 1]).astype(bf16)
    for k in range(NY):
        y = mod(p[1] - k, NY)
        for x in range(NX):
            out[y * NX + x] = result[:, k * OWN + x * ROWS : k * OWN + (x + 1) * ROWS]


def output_kernel(attn, p, *refs):
    rows, refs = (refs[:1], refs[1:]) if attn else (refs[:NX], refs[NX:])
    weights, refs = refs[: NC * NX], refs[NC * NX :]
    out = refs[-1]
    half = weights[0].shape[0]
    total = refs[0][...] if attn else jnp.zeros(out.shape, f32)
    for i in range(NC):
        for r in range(NX):
            if attn:
                head = mod(p[3] + i, NC) * 2
                pair = [rows[0][(head + h) * NX + mod(p[2] - r, NX)] for h in range(2)]
                part = jnp.concatenate(pair, axis=0).T
            else:
                part = rows[r][:, i * half : (i + 1) * half]
            total = total + jnp.dot(part, weights[i * NX + r][...], preferred_element_type=f32)
    out[...] = total.astype(out.dtype)


def local(
    activations,
    in_gain,
    w_pool_in,
    pool_gain,
    w_qlat,
    w_kvlat,
    w_krope,
    qlat_gain,
    kvlat_gain,
    w_qup,
    w_kup,
    w_vup,
    qhead_gain,
    khead_gain,
    w_out_pool,
    w_out_attn,
):
    at_z, at_y, at_x, at_c = (lax.axis_index(a) for a in ("z", "y", "x", "c"))
    place = jnp.stack([at_z, at_y, at_x, at_c]).astype(jnp.int32)

    normed = row_norm(activations, in_gain).astype(bf16)
    arrived = [normed] + [shift(normed, "x", k) for k in range(1, NX)]
    (normed, w_kvlat, w_qlat, w_kup, w_vup, w_qup) = lax.optimization_barrier(
        (normed, w_kvlat, w_qlat, w_kup, w_vup, w_qup)
    )
    token = jnp.arange(OWN, dtype=jnp.int32)
    positions = (at_z * NY + at_y) * WIDE + (token // ROWS) * (NC * ROWS) + at_c * ROWS + token % ROWS

    def beside(w):
        return w, shift(w, "c", 1)

    down, kv_up, q_up = on_chip(
        arrange_kernel,
        (
            struct(KEY_WIDTH + ROPE + QUERY_WIDTH, activations.shape[1]),
            struct(NY * (NOPE + VDIM), KVLAT),
            struct(NY * HEAD, QLAT),
        ),
        place, *beside(w_kvlat), *beside(w_qlat), w_krope, *beside(w_kup), *beside(w_vup), *beside(w_qup),
    )
    frequency = rope_theta ** (-jnp.arange(0, ROPE, 2, dtype=f32) / ROPE)
    angles = frequency[:, None] * positions.astype(f32)[None, :]
    cosine, sine = jnp.cos(angles), jnp.sin(angles)
    kv_gain, q_gain, k_gain, qh_gain = (g[None] for g in (kvlat_gain, qlat_gain, khead_gain, qhead_gain))
    down, cosine, sine, kv_gain, q_gain, k_gain, qh_gain = lax.optimization_barrier(
        (down, cosine, sine, kv_gain, q_gain, k_gain, qh_gain)
    )

    rows, kv_part, rope_key, q_part = on_chip(
        project_kernel,
        (
            struct(OWN, activations.shape[1]),
            struct(KEY_WIDTH, OWN),
            struct(ROPE, OWN),
            struct(QUERY_WIDTH, OWN),
        ),
        place, *arrived, down,
    )

    kv_parts = [kv_part] + [shift(kv_part, "x", k) for k in range(1, NX)]
    key_values = on_chip(
        key_kernel,
        (struct(HEAD + VDIM, OWN),) * NY,
        place, *kv_parts, rope_key, kv_up, kv_gain, k_gain, cosine, sine,
        scratch=(pltpu.VMEM((KVLAT, OWN), f32), pltpu.VMEM((NY * (NOPE + VDIM), OWN), f32)),
    )
    slots = [key_values[0]] + [shift(key_values[k], "y", k) for k in range(1, NY)]
    piece = jnp.stack([jnp.concatenate(slots[:2], axis=1), jnp.concatenate(slots[2:], axis=1)])
    piece, rows = lax.optimization_barrier((piece, rows))

    q_parts = [q_part] + [shift(q_part, "x", k) for k in range(1, NX)]
    queries = on_chip(
        query_kernel,
        (struct(HEAD, OWN),) * NY,
        place, *q_parts, q_up, q_gain, qh_gain, cosine, sine,
        scratch=(pltpu.VMEM((QLAT, OWN), f32), pltpu.VMEM((NY * HEAD, OWN), f32)),
    )
    own_w = jnp.concatenate([w_out_pool, w_out_attn], axis=0)
    weights = [own_w] + [shift(own_w, "x", k) for k in range(1, NX)]
    mine = jnp.concatenate([queries[0]] + [shift(queries[k], "y", k) for k in range(1, NY)], axis=1)
    other = shift(mine, "c", 1)

    pool_cols = jnp.concatenate(beside(w_pool_in), axis=1)
    pool_in = jnp.dot(rows, pool_cols, preferred_element_type=f32).astype(bf16)
    pool_w = pool_in.shape[1]
    strips = pool_in.reshape(NX, ROWS, pool_w)
    tails = strips[:, ROWS - RIM :]
    across = shift(tails, "c", 1)
    route = [((g - 1) * NC + 1, g * NC) for g in range(1, NZ * NY)]
    far = lax.ppermute(tails[NX - 1], ("z", "y", "c"), route)
    across = jnp.concatenate([across[..., pool_w // 2 :], across[..., : pool_w // 2]], axis=-1)
    far = jnp.concatenate([far[..., pool_w // 2 :], far[..., : pool_w // 2]], axis=-1)
    before = jnp.where(at_c == 1, across, jnp.concatenate([far[None], across[: NX - 1]], axis=0))
    sums = jnp.concatenate([before, strips], axis=1).astype(f32)
    pooled_sums = []
    for reach in (1, 2, 4, 8):
        sums = sums[:, reach:] + sums[:, :-reach]
        pooled_sums.append(sums[:, sums.shape[1] - ROWS :])
    chosen = pooled_sums[-1]
    for level in range(3):
        chosen = jnp.where(at_x == level, pooled_sums[level], chosen)
    divisor = jnp.minimum(positions + 1, jnp.left_shift(2, at_x)).astype(f32).reshape(NX, ROWS, 1)
    pooled = chosen / divisor - strips.astype(f32)
    pool_out = (pooled * jnp.concatenate(beside(pool_gain))).astype(bf16)
    pool_rows = [pick(pool_out, at_x)] + [shift(pick(pool_out, (at_x + k) % NX), "x", k) for k in range(1, NX)]
    up, down, state = piece, piece, None
    for step in range(1, NZ // 2):
        up, down = shift(up, "z", 1), shift(down, "z", -1)
        own = [piece] if step == 1 else []
        state = attend(mine, other, own + [up, down], (0,) * len(own) + (-step, step), place, state)
    state, *weights = lax.optimization_barrier((state, *weights))
    weights += [shift(w, "c", 1) for w in weights]
    end = shift(up, "z", 1)
    here, there = attend(mine, other, [end], (NZ // 2,), place, state, last=True)
    there = shift(there, "c", 1)
    pool_term = on_chip(
        lambda *refs: output_kernel(False, *refs),
        struct(ROWS, activations.shape[1], dtype=f32),
        place, *pool_rows, *weights,
        specs=[WHOLE] * NX + [HALVES[0]] * (NC * NX),
    )

    attended = on_chip(merge_kernel, struct(NY * NX, VDIM, ROWS), place, here, there)
    attn_rows = lax.all_to_all(attended, ("y", "x"), 0, 0, tiled=True)
    return on_chip(
        lambda *refs: output_kernel(True, *refs),
        struct(ROWS, activations.shape[1]),
        place, attn_rows, *weights, pool_term,
        specs=[WHOLE] + [HALVES[1]] * (NC * NX) + [WHOLE],
    )


def solution(mesh):
    fine = Mesh(mesh.devices.reshape(NZ, NY, NX, NC), ("z", "y", "x", "c"))
    tp = ("x", "c")
    every = ("z", "y", "x", "c")
    placed = (
        P(every, None),
        P(),
        P(None, tp),
        P(tp),
        P(None, tp),
        P(None, tp),
        P(),
        P(),
        P(),
        P(None, tp),
        P(None, tp),
        P(None, tp),
        P(),
        P(),
        P(tp, None),
        P(tp, None),
    )

    return jax.shard_map(local, mesh=fine, in_specs=placed, out_specs=P(every, None), check_vma=False)
```
